32 devices in a mesh: grp: 2 (over y), sp: 4 (over z), tp: 4 (over x, core).
Axes of the slice: x: 2, y: 2, z: 4, core: 2. Of those that a mesh axis runs over, the one named last changes fastest.
Arguments:
- tokens: bfloat16 [1024, 2048], P(('grp', 'sp'), 'tp'), parts along dimension 0, may hold values from -6 to 6
- norm_gain: float32 [2048], replicated, may hold values from 0.1 to 1.9
- att_q_weight: bfloat16 [1024, 2048], P('tp', 'sp'), may hold values from -0.625 to 0.625
- att_k_weight: bfloat16 [512, 2048], P('tp', 'sp'), may hold values from -0.125 to 0.125
- att_v_weight: bfloat16 [512, 2048], P('tp', 'sp'), may hold values from -0.125 to 0.125
- rec_q_weight: bfloat16 [1024, 2048], P('tp', 'sp'), may hold values from -0.125 to 0.125
- rec_f_weight: bfloat16 [1024, 2048], P('tp', 'sp'), may hold values from -0.125 to 0.125
- rec_i_weight: bfloat16 [1024, 2048], P('tp', 'sp'), may hold values from -0.125 to 0.125
- att_out_weight: bfloat16 [1024, 2048], P('tp', 'sp'), may hold values from -1.5 to 1.5
- rec_out_weight: bfloat16 [1024, 2048], P('tp', 'sp'), may hold values from -0.1875 to 0.1875
- score_offset: float32 [16], P('tp'), may hold values from -11.5 to -3
- lower_bound: float32 [1024], P('tp'), may hold values from 0.94 to 0.99999
- decay_shift: float32 [1024, 1024], P(('grp', 'sp'), 'tp'), parts along dimension 0, may hold values from -2.1 to 0
- rec_gain: float32 [1024], P('tp'), may hold values from 0.1 to 1.9
Outputs:
- mixed: bfloat16 [1024, 2048], P(('grp', 'sp', 'tp')), parts along dimension 0
The draws below stay inside these ranges and needn't reach their ends.
There are 2 independent parts, one for each index of `grp`. The reference program is written for one: setup_inputs(seed, part) draws one part's arguments, and reference() takes and returns one part's arrays. A program takes and returns all parts, laid end to end along the dimension named above; an argument that names none is the same for every part. Nothing has to cross between parts.
All inputs are finite; a program needn't handle non-finite values.
Results may differ from the reference program's by a relative error of at most 0.015.
Values may be sent and summed in bfloat16 or wider, within the bound.
A program may use at most 64 MiB of HBM per device.

```python
import math
import jax
import jax.numpy as jnp
from jax import lax

D = 2048
ATT_HEADS = 16
KV_HEADS = 8
HEAD = 64
RECURRENT_COUNT = 8
REC_KEY = 128
REC_VAL = 128
SPAN = 64
TOK_DEV = 128
SEQ = 512
ATT_WIDTH = 1024
KV_WIDTH = 512
KEY_WIDTH = 1024
VAL_WIDTH = 1024
N_TP = 4


def draw_score_offset(key, part):
    order = jax.random.permutation(jax.random.fold_in(key, 11), ATT_HEADS)
    level = jax.random.uniform(jax.random.fold_in(key, 12), (ATT_HEADS,), jnp.float32)
    slow = order >= ATT_HEADS // 2
    far = -11.5 + 1.5 * level
    near = -6.0 + 3.0 * level
    return jnp.where(slow, far, near).astype(jnp.float32)


def draw_lower_bound(key, part):
    order = jax.random.permutation(jax.random.fold_in(key, 21), RECURRENT_COUNT)
    slow = order >= RECURRENT_COUNT // 2
    level = jax.random.uniform(jax.random.fold_in(key, 22), (RECURRENT_COUNT, REC_KEY), jnp.float32)
    slow_gap = jnp.exp(math.log(1.5e-05) + level * math.log(5e-05 / 1.5e-05))
    fast_gap = jnp.exp(math.log(0.02) + level * math.log(3.0))
    gap = jnp.where(slow[:, None], slow_gap, fast_gap)
    return (1.0 - gap).reshape(KEY_WIDTH).astype(jnp.float32)


def draw_decay_shift(key, part):
    blocks = SEQ // TOK_DEV
    level = jax.random.uniform(jax.random.fold_in(key, 31), (blocks, KEY_WIDTH), jnp.float32)
    rate = jnp.exp(math.log(2.5e-06) + level * math.log(3e-05 / 2.5e-06))
    shift_floor_amount = -jnp.repeat(rate, TOK_DEV, axis=0)
    spots = jax.random.randint(jax.random.fold_in(key, 32), (3,), 0, SEQ)
    leftover_stick = jax.random.uniform(jax.random.fold_in(key, 33), (3, KEY_WIDTH), jnp.float32, 0.2, 0.5)
    stick_fraction = (jnp.arange(SEQ, dtype=jnp.int32)[:, None] == spots[None, :]).astype(jnp.float32)
    segment_tile = jnp.dot(stick_fraction, jnp.log(1.0 - leftover_stick), precision=jax.lax.Precision.HIGHEST)
    return (shift_floor_amount + segment_tile).astype(jnp.float32)


def block_levels(key, extent, cuts, smallest, top_value):
    factor_of, own = 1.0, jax.random.fold_in(key, 6)
    for dim, parts in cuts:
        heights = jnp.exp(jax.random.uniform(jax.random.fold_in(own, dim), (parts,), jnp.float32, smallest / len(cuts), top_value / len(cuts)))
        factor_of = factor_of * jnp.repeat(heights, extent[dim] // parts).reshape([-1 if axis == dim else 1 for axis in range(len(extent))])
    return factor_of


def noise(stream_key, dims, spread, bound, cuts=(), kind=jnp.bfloat16):
    drawn = jax.random.normal(stream_key, dims, jnp.float32) * spread
    if len(cuts) > 0:
        drawn = block_levels(stream_key, dims, cuts, -0.22, 0.18) * drawn
    return jnp.clip(drawn, min=-bound, max=bound).astype(kind)


def setup_inputs(seed: int = 0, part: int = 0) -> dict:
    key_of = jax.random.split(jax.random.key(seed), 15)
    own_keys = jax.random.split(jax.random.fold_in(key_of[14], part), 15)
    return {
        "tokens": noise(own_keys[0], (SEQ, D), 1.0, 6.0, ((0, 4), (1, 4))),
        "norm_gain": jnp.clip(1.0 + 0.18 * jax.random.normal(key_of[1], (D,), jnp.float32), 0.1, 1.9),
        "att_q_weight": noise(key_of[2], (ATT_WIDTH, D), (2 * D ** -0.5), 0.625, ((0, 4), (1, 4))),
        "att_k_weight": noise(key_of[3], (KV_WIDTH, D), D ** -0.5, 0.125, ((0, 4), (1, 4))),
        "att_v_weight": noise(key_of[4], (KV_WIDTH, D), D ** -0.5, 0.125, ((0, 4), (1, 4))),
        "rec_q_weight": noise(key_of[5], (KEY_WIDTH, D), D ** -0.5, 0.125, ((0, 4), (1, 4))),
        "rec_f_weight": noise(key_of[6], (KEY_WIDTH, D), D ** -0.5, 0.125, ((0, 4), (1, 4))),
        "rec_i_weight": noise(key_of[7], (VAL_WIDTH, D), D ** -0.5, 0.125, ((0, 4), (1, 4))),
        "att_out_weight": noise(key_of[8], (ATT_WIDTH, D), (3 * ATT_WIDTH ** -0.5), 1.5, ((0, 4), (1, 4))),
        "rec_out_weight": noise(key_of[9], (VAL_WIDTH, D), VAL_WIDTH ** -0.5, 0.1875, ((0, 4), (1, 4))),
        "score_offset": draw_score_offset(jax.random.fold_in(key_of[14], 71), part),
        "lower_bound": draw_lower_bound(jax.random.fold_in(key_of[14], 71), part),
        "decay_shift": draw_decay_shift(jax.random.fold_in(jax.random.fold_in(key_of[14], part), 71), part),
        "rec_gain": jnp.clip(1.0 + 0.18 * jax.random.normal(key_of[13], (VAL_WIDTH,), jnp.float32), 0.1, 1.9),
    }


EPS = 1e-06
TOP_PRECISION = lax.Precision.HIGHEST

def rounded(values):
    return lax.optimization_barrier(values.astype(jnp.bfloat16))

def block_pass(carry, inputs):
    state_matrix = carry
    query_rows, log_decay, keyed_values, value_rows = inputs
    span = query_rows.shape[0]
    cumulative_log = jnp.cumsum(log_decay, axis=0)
    lower = jnp.arange(span, dtype=jnp.int32)[:, None] >= jnp.arange(span, dtype=jnp.int32)[None, :]
    diff = cumulative_log[:, None] - cumulative_log[None, :]
    decay = jnp.exp(jnp.where(lower[:, :, None, None], diff, -jnp.inf))
    score = jnp.einsum('thk,tshk,shk->ths', query_rows, decay, keyed_values, precision=TOP_PRECISION)
    inner = jnp.einsum('ths,shv->thv', score, value_rows, precision=TOP_PRECISION)
    outer_product = jnp.einsum('ril,ilc->ric', query_rows * jnp.exp(cumulative_log), state_matrix, precision=TOP_PRECISION)
    final_state = cumulative_log[-1]
    state_matrix = state_matrix * jnp.exp(final_state)[:, :, None] + jnp.einsum('iag,iax->agx', keyed_values * jnp.exp(final_state[None] - cumulative_log), value_rows, precision=TOP_PRECISION)
    return (state_matrix, inner + outer_product)

def reference(tokens, norm_gain, att_q_weight, att_k_weight, att_v_weight, rec_q_weight, rec_f_weight, rec_i_weight, att_out_weight, rec_out_weight, score_offset, lower_bound, decay_shift, rec_gain):
    raw = tokens.astype(jnp.float32)
    scaled = (raw * norm_gain[None, :]).astype(jnp.bfloat16)
    inv_rms = lax.rsqrt(lax.optimization_barrier(jnp.mean(raw * raw, axis=1)) + EPS)

    def project(weight):
        return rounded(jnp.dot(scaled, weight.T, preferred_element_type=jnp.float32) * inv_rms[:, None])
    att_query = project(att_q_weight)
    att_key = project(att_k_weight)
    att_value = project(att_v_weight)
    rec_query = project(rec_q_weight)
    rec_forget = project(rec_f_weight)
    rec_input = project(rec_i_weight)
    group = ATT_HEADS // KV_HEADS
    qblock = min(128, SEQ)
    queries = att_query.astype(jnp.float32).reshape(SEQ // qblock, qblock, KV_HEADS, group, HEAD)
    keys = att_key.astype(jnp.float32).reshape(SEQ, KV_HEADS, HEAD)
    values = att_value.astype(jnp.float32).reshape(SEQ, KV_HEADS, HEAD)
    offsets = score_offset.reshape(KV_HEADS, group)
    starts = jnp.arange(SEQ // qblock, dtype=jnp.int32) * qblock
    key_pos = jnp.arange(SEQ, dtype=jnp.int32)

    def attend(args):
        query_block, first = args
        score = jnp.einsum('tkgd,skd->tkgs', query_block, keys, precision=TOP_PRECISION) * HEAD ** (-0.5) + offsets[None, :, :, None]
        query_pos = first + jnp.arange(qblock, dtype=jnp.int32)
        visible = (key_pos[None, :] < query_pos[:, None])[:, None, None, :]
        keep = jnp.where(visible, jax.nn.log_sigmoid(-score), 0.0)
        tail = lax.cumsum(keep, axis=3, reverse=True) - keep
        weight = jnp.where(visible, jnp.exp(jax.nn.log_sigmoid(score) + tail), 0.0)
        weight = rounded(weight).astype(jnp.float32)
        return jnp.einsum('tkgs,skd->tkgd', weight, values, precision=TOP_PRECISION)
    att_out = lax.map(attend, (queries, starts)).reshape(SEQ, ATT_WIDTH).astype(jnp.bfloat16)
    logit = rec_forget.astype(jnp.float32)
    gap = 1.0 - lower_bound
    log_decay = jnp.log(lower_bound + gap * jax.nn.sigmoid(logit)) + decay_shift
    keyed_values = gap * jax.nn.sigmoid(-logit)
    rec_q = jax.nn.silu(rec_query.astype(jnp.float32))
    blocks = SEQ // SPAN

    def split(array, depth):
        return array.reshape(blocks, SPAN, RECURRENT_COUNT, depth)
    start_state = jnp.zeros((RECURRENT_COUNT, REC_KEY, REC_VAL), jnp.float32)
    _, rec_raw = lax.scan(block_pass, start_state, (split(rec_q, REC_KEY), split(log_decay, REC_KEY), split(keyed_values, REC_KEY), split(rec_input.astype(jnp.float32), REC_VAL)))
    rec_raw = rec_raw.reshape(SEQ, RECURRENT_COUNT, REC_VAL)
    rescaled_input = rec_raw * lax.rsqrt(lax.optimization_barrier(jnp.mean(rec_raw * rec_raw, axis=2, keepdims=True)) + EPS) * rec_gain.reshape(RECURRENT_COUNT, REC_VAL)
    rec_out = rescaled_input.reshape(SEQ, VAL_WIDTH).astype(jnp.bfloat16)
    att_cols = ATT_WIDTH // N_TP
    rec_cols = VAL_WIDTH // N_TP
    total = jnp.zeros((SEQ, D), jnp.float32)
    for group_index in range(N_TP):
        att_part = att_out[:, group_index * att_cols:(group_index + 1) * att_cols]
        rec_part = rec_out[:, group_index * rec_cols:(group_index + 1) * rec_cols]
        partial_value = jnp.dot(att_part, att_out_weight[group_index * att_cols:(group_index + 1) * att_cols], preferred_element_type=jnp.float32)
        partial_value = partial_value + jnp.dot(rec_part, rec_out_weight[group_index * rec_cols:(group_index + 1) * rec_cols], preferred_element_type=jnp.float32)
        total = total + rounded(partial_value).astype(jnp.float32)
    return total.astype(jnp.bfloat16)
```

```python
import contextlib
import functools

import jax
import jax.numpy as jnp
from jax import lax
from jax.experimental import pallas as pl
from jax.experimental.pallas import tpu as pltpu
from jax.sharding import PartitionSpec as P

HEAD = 64
REC_KEY = 128
REC_VAL = 128
SPAN = 64


EPS = 1e-06
TOP_PRECISION = lax.Precision.HIGHEST


def entering(x, axis, combine, identity):
    count, here = (lax.axis_size(axis), lax.axis_index(axis))
    everything = jax.tree.map(
        lambda part, kind: lax.all_gather(part.astype(kind), axis), x, (jnp.bfloat16, jnp.bfloat16)
    )
    start = jax.tree.map(
        lambda part, zero: jnp.broadcast_to(jnp.asarray(zero, part.dtype), part.shape), x, identity
    )

    def entering_turn(k, before):
        reached = k < here
        new = combine(
            before, jax.tree.map(lambda part, own: part[k].astype(own.dtype), everything, x)
        )
        return jax.tree.map(lambda a, b: jnp.where(reached, a, b), new, before)

    return lax.fori_loop(0, count, entering_turn, start)


def make_fold(norm_gain, weights, carry, piece):
    elementwise_sq, totals = carry
    raw = piece.astype(jnp.float32)
    scaled = (raw * norm_gain[None, :]).astype(jnp.bfloat16)
    elementwise_sq = jnp.sum(raw * raw, axis=1)
    updated = []
    for total, weight in zip(totals, weights):
        updated.append(
            lax.dot_general(
                scaled, weight, (((1,), (1,)), ((), ())), preferred_element_type=jnp.float32
            )
        )
    return (elementwise_sq, tuple(updated))


def project_all(tokens, norm_gain, weights):
    rows = tokens.shape[0]
    width = weights[0].shape[1]
    start_carry = (
        jnp.zeros((rows,), jnp.float32),
        tuple((jnp.zeros((rows, weight.shape[0]), jnp.float32) for weight in weights)),
    )
    elementwise_sq, totals = make_fold(
        norm_gain, weights, start_carry, lax.all_gather(tokens, "tp", axis=1, tiled=True)
    )
    inv_rms = lax.rsqrt(elementwise_sq / width + EPS)
    return tuple((total * inv_rms[:, None] for total in totals))


def attention(att_query, key_value, score_offset):
    rows = att_query.shape[0]
    gathered = lax.all_gather(key_value, "sp", axis=0, tiled=True)
    seq = gathered.shape[0]
    kv_heads = key_value.shape[1] // (2 * HEAD)
    q_heads = att_query.shape[1] // HEAD
    group = q_heads // kv_heads
    kv_width = kv_heads * HEAD
    queries = att_query.reshape(rows, kv_heads, group, HEAD)
    offsets = score_offset.reshape(kv_heads, group)
    kblock = min(1024, seq)
    first_row = lax.axis_index("sp") * rows
    query_pos = first_row + jnp.arange(rows, dtype=jnp.int32)
    count = (first_row + rows - 1) // kblock + 1

    def attention_turn(step, carry):
        summed, run = carry
        block_start = (count - 1 - step) * kblock
        block = lax.dynamic_slice_in_dim(gathered, block_start, kblock, 0)
        keys = block[:, :kv_width].reshape(kblock, kv_heads, HEAD)
        values = block[:, kv_width:].reshape(kblock, kv_heads, HEAD)
        score = (
            jnp.einsum("tkgd,skd->tkgs", queries, keys, preferred_element_type=jnp.float32)
            * HEAD ** (-0.5)
            + offsets[None, :, :, None]
        )
        key_pos = block_start + jnp.arange(kblock, dtype=jnp.int32)
        visible = (key_pos[None, :] < query_pos[:, None])[:, None, None, :]
        keep = jnp.where(visible, jax.nn.log_sigmoid(-score), 0.0)
        tail = lax.cumsum(keep, axis=3, reverse=True) - keep
        weight = jnp.where(
            visible, jnp.exp(jax.nn.log_sigmoid(score) + tail + run[..., None]), 0.0
        ).astype(jnp.bfloat16)
        summed = summed + jnp.einsum(
            "tkgs,skd->tkgd", weight, values, preferred_element_type=jnp.float32
        )
        return (summed, run + jnp.sum(keep, axis=3))

    start_carry = (
        jnp.zeros((rows, kv_heads, group, HEAD), jnp.float32),
        jnp.zeros((rows, kv_heads, group), jnp.float32),
    )
    summed, _ = lax.fori_loop(0, count, attention_turn, start_carry)
    return summed.reshape(rows, q_heads * HEAD).astype(jnp.bfloat16)


def block_pass(carry, inputs):
    state_matrix, prefix = carry
    query_rows, log_decay, keyed_values, value_rows = inputs
    span = query_rows.shape[0]
    cumulative_log = jnp.cumsum(log_decay, axis=0)
    lower = jnp.arange(span, dtype=jnp.int32)[:, None] >= jnp.arange(span, dtype=jnp.int32)[None, :]
    diff = cumulative_log[:, None] - cumulative_log[None, :]
    decay = jnp.exp(jnp.where(lower[:, :, None, None], diff, -jnp.inf))
    score = jnp.einsum(
        "thk,tshk,shk->ths", query_rows, decay, keyed_values, precision=TOP_PRECISION
    )
    inner = jnp.einsum("ths,shv->thv", score, value_rows, precision=TOP_PRECISION)
    outer_product = jnp.einsum(
        "ril,ilc->ric", query_rows * jnp.exp(cumulative_log), state_matrix, precision=TOP_PRECISION
    )
    final_state = cumulative_log[-1]
    state_matrix = state_matrix * jnp.exp(final_state)[:, :, None] + jnp.einsum(
        "iag,iax->agx",
        keyed_values * jnp.exp(final_state[None] - cumulative_log),
        value_rows,
        precision=TOP_PRECISION,
    )
    reach_limit = query_rows * jnp.exp(cumulative_log + prefix[None])
    return ((state_matrix, prefix + final_state), (inner + outer_product, reach_limit))


def chain(earlier, later):
    return (earlier[0] * later[0], earlier[1] * later[0][:, :, None] + later[1])


def recurrence(rec_query, rec_forget, rec_input, lower_bound, decay_shift, rec_gain):
    rows = rec_query.shape[0]
    heads = rec_gain.shape[0] // REC_VAL
    logit = rec_forget.astype(jnp.float32)
    gap = 1.0 - lower_bound
    log_decay = jnp.log(lower_bound + gap * jax.nn.sigmoid(logit)) + decay_shift
    keyed_values = gap * jax.nn.sigmoid(-logit)
    query_rows = jax.nn.silu(rec_query.astype(jnp.float32))
    blocks = rows // SPAN

    def split(array, depth):
        return array.reshape(blocks, SPAN, heads, depth)

    start_carry = (
        jnp.zeros((heads, REC_KEY, REC_VAL), jnp.float32),
        jnp.zeros((heads, REC_KEY), jnp.float32),
    )
    (state_matrix, total), (local, reach_limit) = lax.scan(
        block_pass,
        start_carry,
        (
            split(query_rows, REC_KEY),
            split(log_decay, REC_KEY),
            split(keyed_values, REC_KEY),
            split(rec_input.astype(jnp.float32), REC_VAL),
        ),
    )
    identity = (
        jnp.ones((heads, REC_KEY), jnp.float32),
        jnp.zeros((heads, REC_KEY, REC_VAL), jnp.float32),
    )
    incoming_state = entering((jnp.exp(total), state_matrix), "sp", chain, identity)
    running_memory = jnp.einsum(
        "lida,dao->lido", reach_limit, incoming_state[1], precision=TOP_PRECISION
    )
    rec_raw = (local + running_memory).reshape(rows, heads, REC_VAL)
    rescaled_input = (
        rec_raw
        * lax.rsqrt(jnp.mean(rec_raw * rec_raw, axis=2, keepdims=True) + EPS)
        * rec_gain.reshape(heads, REC_VAL)
    )
    return rescaled_input.reshape(rows, heads * REC_VAL).astype(jnp.bfloat16)


def gathered_plan(
    tokens,
    norm_gain,
    att_q_weight,
    att_k_weight,
    att_v_weight,
    rec_q_weight,
    rec_f_weight,
    rec_i_weight,
    att_out_weight,
    rec_out_weight,
    score_offset,
    lower_bound,
    decay_shift,
    rec_gain,
):
    inputs = (
        lax.all_gather(att_q_weight, "sp", axis=1, tiled=True),
        lax.all_gather(att_k_weight, "sp", axis=1, tiled=True),
        lax.all_gather(att_v_weight, "sp", axis=1, tiled=True),
        lax.all_gather(rec_q_weight, "sp", axis=1, tiled=True),
        lax.all_gather(rec_f_weight, "sp", axis=1, tiled=True),
        lax.all_gather(rec_i_weight, "sp", axis=1, tiled=True),
    )
    projected = project_all(tokens, norm_gain, inputs)
    att_query = projected[0].astype(jnp.bfloat16)
    key_value = jnp.concatenate(projected[1:3], axis=1).astype(jnp.bfloat16)
    rec_query = projected[3].astype(jnp.bfloat16)
    rec_forget = projected[4].astype(jnp.bfloat16)
    rec_input = projected[5].astype(jnp.bfloat16)
    att_out = attention(att_query, key_value, score_offset)
    rec_out = recurrence(rec_query, rec_forget, rec_input, lower_bound, decay_shift, rec_gain)
    outputs = (
        lax.all_gather(att_out_weight, "sp", axis=1, tiled=True),
        lax.all_gather(rec_out_weight, "sp", axis=1, tiled=True),
    )
    att_rows, rec_rows = outputs
    return lax.psum_scatter(
        (
            jnp.dot(att_out, att_rows, preferred_element_type=jnp.float32)
            + jnp.dot(rec_out, rec_rows, preferred_element_type=jnp.float32)
        ).astype(jnp.bfloat16),
        "tp",
        scatter_dimension=0,
        tiled=True,
    )


MESH = pl.DeviceIdType.MESH
STEP = 32


def dot_nt(a, b):
    return lax.dot_general(a, b, (((1,), (1,)), ((), ())), preferred_element_type=jnp.float32)


def dot_tn(a, b):
    return lax.dot_general(a, b, (((0,), (0,)), ((), ())), preferred_element_type=jnp.float32)


def dot_nn(a, b):
    return jnp.dot(a, b, preferred_element_type=jnp.float32)


def remote(src, dst, send_sem, recv_sem, target):
    return pltpu.make_async_remote_copy(
        src_ref=src,
        dst_ref=dst,
        send_sem=send_sem,
        recv_sem=recv_sem,
        device_id=target,
        device_id_type=MESH,
    )


SUB = 32
ROWS8 = 8
LAST = 64
PROFILE = False


def scope(name):
    return jax.named_scope(name) if PROFILE else contextlib.nullcontext()


def stick_block(first, rows, j, group, x, offset_ref):
    block = 128
    q, base = first // block, first % block
    low = lax.broadcasted_iota(jnp.int32, (block, block), 0)
    high = lax.broadcasted_iota(jnp.int32, (block, block), 1)
    later = (low > high).astype(jnp.bfloat16)
    row = lax.broadcasted_iota(jnp.int32, (rows, block), 0) + base
    col = lax.broadcasted_iota(jnp.int32, (rows, block), 1)
    visible = jnp.concatenate([col < row] * group, axis=0)
    offset = jnp.concatenate(
        [jnp.full((rows, block), offset_ref[j * group + g], jnp.float32) for g in range(group)],
        axis=0,
    )
    queries = x[first:first + rows, :group * HEAD]
    queries = jnp.concatenate([queries[:, g * HEAD:(g + 1) * HEAD] for g in range(group)], axis=0)
    run = jnp.zeros((group * rows, 1), jnp.float32)
    summed = jnp.zeros((group * rows, HEAD), jnp.float32)
    for c in range(q, -1, -1):
        keys = x[c * block:(c + 1) * block, group * HEAD:(group + 1) * HEAD]
        values = x[c * block:(c + 1) * block, (group + 1) * HEAD:(group + 2) * HEAD]
        score = dot_nt(queries, keys) * HEAD ** (-0.5) + offset
        keep = -(jnp.maximum(score, 0.0) + jnp.log1p(jnp.exp(-jnp.abs(score))))
        gate = score + keep
        if c == q:
            keep = jnp.where(visible, keep, 0.0)
        top = keep.astype(jnp.bfloat16)
        rest = (keep - top.astype(jnp.float32)).astype(jnp.bfloat16)
        tail = dot_nn(top, later) + dot_nn(rest, later)
        weight = jnp.exp(gate + tail + run)
        if c == q:
            weight = jnp.where(visible, weight, 0.0)
        summed = summed + dot_nn(weight.astype(jnp.bfloat16), values)
        run = run + jnp.sum(keep, axis=1, keepdims=True)
    return jnp.concatenate(
        [summed[g * rows:(g + 1) * rows] for g in range(group)], axis=1
    ).astype(jnp.bfloat16)


def state_block(begin, rows, x, first, bound, gain, shift_ref, state_ref):
    gap = 1.0 - bound
    low = lax.broadcasted_iota(jnp.int32, (rows, rows), 0)
    high = lax.broadcasted_iota(jnp.int32, (rows, rows), 1)
    upto = ((high <= low) & (high // STEP == low // STEP)).astype(jnp.float32)
    lower = (
        lax.broadcasted_iota(jnp.int32, (STEP, STEP), 0)
        >= lax.broadcasted_iota(jnp.int32, (STEP, STEP), 1)
    )
    state = jnp.zeros((REC_VAL, REC_KEY), jnp.float32) if begin == 0 else state_ref[...]
    at = slice(begin, begin + rows)
    query = x[at, first:first + REC_KEY].astype(jnp.float32)
    logit = x[at, first + REC_KEY:first + 2 * REC_KEY].astype(jnp.float32)
    value = x[at, first + 2 * REC_KEY:first + 2 * REC_KEY + REC_VAL]
    log_decay = jnp.log(bound + gap * jax.nn.sigmoid(logit)) + shift_ref[at]
    keyed = gap * jax.nn.sigmoid(-logit)
    query = query * jax.nn.sigmoid(query)
    running = jnp.dot(upto, log_decay, precision=TOP_PRECISION, preferred_element_type=jnp.float32)
    outs = []
    for i in range(rows // STEP):
        it = slice(i * STEP, (i + 1) * STEP)
        cumulative, q, k, v = running[it], query[it], keyed[it], value[it]
        middle = cumulative[STEP // 2 - 1:STEP // 2]
        last = cumulative[STEP - 1:STEP]
        score = dot_nt(
            (q * jnp.exp(cumulative - middle)).astype(jnp.bfloat16),
            (k * jnp.exp(middle - cumulative)).astype(jnp.bfloat16),
        )
        score = jnp.where(lower, score, 0.0).astype(jnp.bfloat16)
        raw = dot_nn(score, v) + dot_nt(
            (q * jnp.exp(cumulative)).astype(jnp.bfloat16), state.astype(jnp.bfloat16)
        )
        state = state * jnp.exp(last) + dot_tn(
            v, (k * jnp.exp(last - cumulative)).astype(jnp.bfloat16)
        )
        scale = lax.rsqrt(jnp.mean(raw * raw, axis=1, keepdims=True) + EPS)
        outs.append((raw * scale * gain).astype(jnp.bfloat16))
    state_ref[...] = state
    return jnp.concatenate(outs, axis=0)


def units_of(n, rows):
    whole = [(k * rows, rows) for k in range(n - 1)]
    return whole + [((n - 1) * rows + r, LAST) for r in range(0, rows, LAST)]


def layer_kernel(
    n, nt, group,
    tok_ref, gain_ref, aq_ref, ak_ref, av_ref, rq_ref, rf_ref, ri_ref, shift_ref,
    wa_ref, wr_ref, offset_ref, bound_ref, rec_gain_ref,
    out_ref,
    tokens, gains, bounds, rec_gains, weights, outs, own_shift, tbuf, shifts, squares, scales,
    part, sent, came, x, state, heads, shares, landed, mixed,
    l_sem, a_send, a_recv, a_local, b_send, b_recv, d_send, d_recv, d_local, q_send, q_recv,
    c_send, c_recv, e_send, e_recv, f_send, f_recv, g_send, g_recv, g_local,
):
    s, t = lax.axis_index("sp"), lax.axis_index("tp")
    rows, feats = own_shift.shape[0], tokens.shape[-1]
    piece = rows // nt
    width = x.shape[1]
    att_width = (group + 2) * HEAD
    wide = group * HEAD
    cols = outs.shape[-1]
    subs = rows // SUB
    ends = (0, n - 1)
    f32, bf16 = jnp.float32, jnp.bfloat16
    units = units_of(n, rows)
    nu = len(units)

    loads = [
        pltpu.make_async_copy(tok_ref, tokens, l_sem.at[0]),
        pltpu.make_async_copy(
            gain_ref.at[:, pl.ds(pl.multiple_of(s * feats, feats), feats)], gains, l_sem.at[1]
        ),
    ]
    first = 0
    for ref, size in (
        (aq_ref, wide), (ak_ref, HEAD), (av_ref, HEAD),
        (rq_ref, REC_KEY), (rf_ref, REC_KEY), (ri_ref, REC_VAL),
    ):
        for i in range(2):
            loads.append(
                pltpu.make_async_copy(
                    ref.at[pl.ds(i * size, size)], weights.at[i, pl.ds(first, size)],
                    l_sem.at[len(loads)],
                )
            )
        first += size
    early = len(loads)
    loads.append(pltpu.make_async_copy(shift_ref, own_shift, l_sem.at[early]))
    loads.append(pltpu.make_async_copy(bound_ref, bounds, l_sem.at[early + 1]))
    loads.append(pltpu.make_async_copy(rec_gain_ref, rec_gains, l_sem.at[early + 2]))
    loads.append(pltpu.make_async_copy(wa_ref, outs.at[0], l_sem.at[early + 3]))
    loads.append(pltpu.make_async_copy(wr_ref, outs.at[1], l_sem.at[early + 4]))

    loads[0].start()
    barrier = pltpu.get_barrier_semaphore()
    for a in range(n):
        for b in range(nt):
            if a or b:
                pl.semaphore_signal(
                    barrier, inc=1,
                    device_id={"sp": lax.rem(s + a, n), "tp": lax.rem(t + b, nt)},
                    device_id_type=MESH,
                )
    for load in loads[1:]:
        load.start()
    loads[0].wait()
    with scope("barrier"):
        pl.semaphore_wait(barrier, n * nt - 1)

    def plane(v):
        others = [i for i in range(2) if v != ends[i]]
        mine = [i for i in range(2) if v == ends[i]]
        order = (1, 0) if v < n // 2 else (0, 1)

        def parts_of(k):
            return range(subs) if k == 0 else (slice(None),)

        def slot(c):
            return 0 if isinstance(c, slice) else c

        def first_copy(c, j):
            return remote(
                tokens.at[c, j], tbuf.at[v, c, j], a_send.at[slot(c), j], a_recv.at[v, slot(c)],
                {"sp": t, "tp": j},
            )

        def first_here(c):
            return pltpu.make_async_copy(
                tokens.at[c, v], tbuf.at[v, c, v], a_local.at[slot(c)]
            )

        def send_first():
            for c in parts_of(v):
                for j in range(nt):
                    if j == v:
                        pl.when(t != v)(lambda: first_copy(c, j).start())
                        pl.when(t == v)(lambda: first_here(c).start())
                    else:
                        first_copy(c, j).start()

        def second_copy(k, c, d):
            return remote(
                tbuf.at[k, c, t], tbuf.at[k, c, t],
                b_send.at[k, slot(c), d], b_recv.at[k, slot(c), d],
                {"tp": lax.rem(t + d, nt)},
            )

        def relay(k, c):
            def arrived():
                remote(
                    tokens.at[c, 0], tbuf.at[k, c, t], a_send.at[0, 0], a_recv.at[k, slot(c)],
                    {"sp": (v + 1) % n},
                ).wait_recv()

            with scope(f"relay{k}"):
                if k == v:
                    pl.when(t != v)(arrived)
                    pl.when(t == v)(lambda: first_here(c).wait())
                else:
                    arrived()
            for d in range(1, nt):
                second_copy(k, c, d).start()

        def square_copy(k, i):
            return remote(
                squares.at[v, k], squares.at[v, k], q_send.at[k, i], q_recv.at[v, k],
                {"sp": ends[i]},
            )

        def chain_copy(i, c):
            to = v - 1 if i == 0 else v + 1
            return remote(
                sent.at[i, pl.ds(c * SUB, SUB)], came.at[i, pl.ds(c * SUB, SUB)],
                c_send.at[i, c], c_recv.at[i, c], {"sp": to},
            )

        def project(k, c):
            with scope(f"wtok{k}"):
                for d in range(1, nt):
                    second_copy(k, c, d).wait_recv()
            size = rows if isinstance(c, slice) else SUB
            begin = k * rows + slot(c) * SUB
            raw = tbuf[k, c].reshape(size, feats).astype(f32)
            scaled = (raw * gains[...]).astype(bf16)
            for i in order:
                product = dot_nt(scaled, weights[i])
                if v == ends[1 - i]:
                    for r in range(size // SUB):
                        at = begin + r * SUB
                        sent[i, pl.ds(at, SUB)] = product[r * SUB:(r + 1) * SUB].astype(bf16)
                        chain_copy(i, at // SUB).start()
                else:
                    part[i, pl.ds(begin, size)] = product

        def square(k):
            raw = tbuf[k].reshape(rows, feats).astype(f32)
            total = jnp.sum(raw * raw, axis=1, keepdims=True)
            flat = jnp.transpose(jnp.broadcast_to(total, (rows, 128)))
            squares[v, k] = flat[:8]
            for i in others:
                square_copy(k, i).start()

        def shift_copy(i):
            return remote(
                own_shift.at[:, pl.ds(i * REC_KEY, REC_KEY)], shifts.at[pl.ds(v * rows, rows)],
                d_send.at[i], d_recv.at[v], {"sp": ends[i]},
            )

        def shift_here(i):
            return pltpu.make_async_copy(
                own_shift.at[:, pl.ds(i * REC_KEY, REC_KEY)], shifts.at[pl.ds(v * rows, rows)],
                d_local,
            )

        def send_shift():
            for i in others:
                shift_copy(i).start()
            for i in mine:
                shift_here(i).start()

        def forward(i, c):
            with scope(f"chain{i}_{c}"):
                chain_copy(i, c).wait_recv()
            at = (i, pl.ds(c * SUB, SUB))
            sent[at] = (part[at] + came[at].astype(f32)).astype(bf16)
            chain_copy(i, c).start()

        def head_copy(i, u, to):
            at = (i, pl.ds(units[u][0], units[u][1]))
            return remote(
                heads.at[at], heads.at[at], e_send.at[u, to], e_recv.at[i, u], {"sp": to}
            )

        def near(i):
            return 1 if i == 0 else n - 2

        def between(i):
            return [p for p in range(1, n - 1) if p != near(i)]

        def direct(u):
            return units[u][1] == LAST

        def head_targets(i, u):
            if v == ends[i]:
                far = ends[1 - i]
                if direct(u):
                    return [far, *between(i), near(i)]
                return [far, near(i)]
            if v == near(i) and not direct(u):
                return between(i)
            return []

        def send_heads(i, u, to):
            head_copy(i, u, to).start()

        def wait_heads(i, u):
            with scope(f"whead{i}_{u}"):
                head_copy(i, u, ends[i]).wait_recv()

        def mix(u):
            e = mine[0]
            begin, size = units[u]
            k = begin // rows
            span = pl.ds(begin, size)
            with scope(f"wmix{u}"):
                for c in range(begin // SUB, (begin + size) // SUB):
                    chain_copy(e, c).wait_recv()
            if begin % rows == 0:
                for p in range(n):
                    if p != v:
                        remote(
                            squares.at[p, k], squares.at[p, k], q_send.at[k, e], q_recv.at[p, k],
                            {"sp": p},
                        ).wait_recv()
                if k == v:
                    shift_here(e).wait()
                else:
                    remote(
                        own_shift.at[:, pl.ds(e * REC_KEY, REC_KEY)],
                        shifts.at[pl.ds(k * rows, rows)], d_send.at[e], d_recv.at[k], {"sp": k},
                    ).wait_recv()
                total = squares[0, k, :1]
                for p in range(1, n):
                    total = total + squares[p, k, :1]
                inv_rms = lax.rsqrt(total / (feats * n) + EPS)
                scales[...] = jnp.transpose(jnp.broadcast_to(inv_rms, (128, rows)))
            inv_rms = scales[pl.ds(begin % rows, size)]
            for c in range(width // 128):
                lane = pl.ds(c * 128, 128)
                result = part[e, span, lane] + came[e, span, lane].astype(f32)
                x[span, lane] = (result * inv_rms).astype(bf16)
            with scope(f"stick{u}"):
                heads[e, span, pl.ds(0, wide)] = stick_block(
                    begin, size, e, group, x, offset_ref
                )
            with scope(f"state{u}"):
                heads[e, span, pl.ds(wide, REC_VAL)] = state_block(
                    begin, size, x, att_width,
                    bounds[:, pl.ds(e * REC_KEY, REC_KEY)],
                    rec_gains[:, pl.ds(e * REC_VAL, REC_VAL)], shifts, state,
                )

        def share_copy(k, b):
            to = lax.rem(t + b, nt)
            return remote(
                shares.at[k, to], landed.at[k, b], f_send.at[k, b], f_recv.at[k, b], {"tp": to}
            )

        def multiply(u):
            begin, size = units[u]
            k = begin // rows
            span = pl.ds(begin, size)
            total = None
            for i in range(2):
                for o, at, deep in ((0, 0, wide), (1, wide, REC_VAL)):
                    term = dot_nn(heads[i, span, pl.ds(at, deep)], outs[o, pl.ds(i * deep, deep)])
                    total = term if total is None else total + term
            total = total.astype(bf16)
            if size == rows:
                shares[k] = total.reshape(nt, piece, cols)
                for b in range(1, nt):
                    share_copy(k, b).start()
            else:
                for j in range(begin % rows // piece, (begin % rows + size) // piece):
                    at = j * piece - begin % rows
                    shares[k, j] = total[at:at + piece]
                    b = lax.rem(j - t + nt, nt)
                    pl.when(t != j)(lambda: share_copy(k, b).start())

        place = out_ref.at[:, pl.ds(v * cols, cols)]

        def final_copy(k):
            return remote(mixed.at[k], place, g_send.at[k], g_recv.at[v], {"sp": k})

        def final_here():
            return pltpu.make_async_copy(mixed.at[v], place, g_local)

        def combine(k):
            with scope(f"wshare{k}"):
                for b in range(1, nt):
                    share_copy(k, b).wait_recv()
            result = shares[k, t].astype(f32)
            for b in range(1, nt):
                result = result + landed[k, b].astype(f32)
            mixed[k] = result.astype(bf16)
            if k == v:
                final_here().start()
            else:
                final_copy(k).start()

        def loaded(first, last):
            for load in loads[first:last]:
                load.wait()

        events = []

        def event(time, *call):
            events.append((time, len(events), call))

        starts = (START0, START1)
        hops = (n - 1 - v, v)
        whole = slice(None)
        event(5.9, loaded, 1, early)
        event(6.9, loaded, early, early + 1)
        event(15.0, loaded, early + 1, len(loads))
        if v == 0:
            event(0.0, send_first)
        for c in range(subs):
            event(4.0 + 0.1 * c, relay, 0, c)
        if v > 0:
            event(4.05, send_first)
        for c in range(subs):
            event(6.0 + 0.1 * c, project, 0, c)
        event(7.0, send_shift)
        event(7.1, square, 0)
        ready = [6.5]
        for k in range(1, n):
            event(6.05 if k == 1 else 9.0 + 0.1 * k, relay, k, whole)
            at = TOKENS + TOKEN_STEP * (k - 1)
            event(at, project, k, whole)
            event(at + 0.1, square, k)
            ready.append(at + 0.01)
        chain_end = 0.0
        if v not in ends:
            for i in range(2):
                for c in range(n * subs):
                    at = max(starts[i] + hops[i] * HOP + CHUNK * c, ready[c // subs])
                    event(at, forward, i, c)
                    chain_end = max(chain_end, at)
        done = [[0.0] * nu, [0.0] * nu]
        for i in range(2):
            at = 0.0
            for u, (begin, size) in enumerate(units):
                last = (begin + size) // SUB - 1
                arrive = max(at, starts[i] + (n - 1) * HOP + CHUNK * last)
                at = arrive + (2.2 if size == rows else 1.6)
                done[i][u] = at
                if v == ends[i]:
                    event(arrive, mix, u)
                    for to in head_targets(i, u):
                        late = 0.0
                        if u == 0 and to == ends[1 - i]:
                            late = 2 * CHUNK * subs
                        event(at - 0.1 + late, send_heads, i, u, to)
        for u, (begin, size) in enumerate(units):
            k = begin // rows
            latest = max(done[0][u], done[1][u])
            for i in others:
                if direct(u):
                    at = done[i][u] + 5.0
                elif v == near(i):
                    at = done[i][u] + 4.2
                elif v == ends[1 - i]:
                    at = done[i][u] + 5.0 + (2 * CHUNK * subs if u == 0 else 0.0)
                else:
                    at = done[i][u] + 8.4
                at = max(at, chain_end)
                event(at, wait_heads, i, u)
                for to in head_targets(i, u):
                    event(at, send_heads, i, u, to)
                latest = max(latest, at)
            event(latest + 0.1, multiply, u)
            if begin + size == (k + 1) * rows:
                event(latest + 4.0, combine, k)
        for _, _, (call, *args) in sorted(events, key=lambda e: e[:2]):
            call(*args)

        for p in range(n):
            if p == v:
                continue
            with scope(f"wfinal{p}"):
                remote(
                    mixed.at[0], out_ref.at[:, pl.ds(p * cols, cols)], g_send.at[0], g_recv.at[p],
                    {"sp": p},
                ).wait_recv()
        with scope("wlocal"):
            final_here().wait()

        with scope("wsend"):
            for c in parts_of(v):
                for j in range(nt):
                    if j == v:
                        pl.when(t != v)(lambda: first_copy(c, j).wait_send())
                    else:
                        first_copy(c, j).wait_send()
            for i in others:
                shift_copy(i).wait_send()
            for k in range(n):
                for d in range(1, nt):
                    for c in parts_of(k):
                        second_copy(k, c, d).wait_send()
                    if k < n - 1:
                        share_copy(k, d).wait_send()
                    else:
                        share_copy(k, d).wait_send()
                for i in others:
                    square_copy(k, i).wait_send()
                    for r in range(subs):
                        chain_copy(i, k * subs + r).wait_send()
                if k != v:
                    final_copy(k).wait_send()
            for i in range(2):
                for u in range(nu):
                    for to in head_targets(i, u):
                        head_copy(i, u, to).wait_send()

    for v in range(n):
        if v in ends:
            @pl.when(s == v)
            def _():
                x[pl.ds((n - 1) * rows, rows)] = jnp.zeros((rows, width), bf16)
                plane(v)
        else:
            pl.when(s == v)(functools.partial(plane, v))


START0, START1, HOP, CHUNK = 8.0, 6.0, 3.4, 0.88
TOKENS, TOKEN_STEP = 10.5, 1.0


def stationary_fits(args):
    n, nt = lax.axis_size("sp"), lax.axis_size("tp")
    tokens, att_q, att_k, rec_i = args[0], args[2], args[3], args[7]
    rows, feats = tokens.shape
    return (
        n == nt
        and n >= 3
        and att_k.shape[0] // HEAD == 2
        and rec_i.shape[0] // REC_VAL == 2
        and (att_q.shape[0] // att_k.shape[0]) * HEAD == 128
        and feats == att_q.shape[1]
        and rows == 128
        and rows == SUB * nt
        and SUB == ROWS8 * nt
    )


def stationary(*args):
    n, nt = lax.axis_size("sp"), lax.axis_size("tp")
    tokens, norm_gain, att_q, att_k = args[:4]
    score_offset, lower_bound, decay_shift, rec_gain = args[10:]
    rows, feats = tokens.shape
    seq = rows * n
    deep, cols = args[8].shape
    group = att_q.shape[0] // att_k.shape[0]
    width = (group + 2) * HEAD + 2 * REC_KEY + REC_VAL
    wide = group * HEAD + REC_VAL
    piece = rows // nt
    chunks = seq // SUB
    subs = rows // SUB
    nu = len(units_of(n, rows))
    bf16, f32 = jnp.bfloat16, jnp.float32
    dma = pltpu.SemaphoreType.DMA
    vmem = pl.BlockSpec(memory_space=pltpu.VMEM)
    hbm = pl.BlockSpec(memory_space=pl.ANY)
    smem = pl.BlockSpec(memory_space=pltpu.SMEM)
    return pl.pallas_call(
        functools.partial(layer_kernel, n, nt, group),
        out_shape=jax.ShapeDtypeStruct((piece, cols * n), bf16),
        in_specs=[hbm] * 11 + [smem, hbm, hbm],
        out_specs=hbm,
        scratch_shapes=[
            pltpu.VMEM((subs, nt, ROWS8, feats), bf16),
            pltpu.VMEM((1, feats), f32),
            pltpu.VMEM((1, 2 * REC_KEY), f32),
            pltpu.VMEM((1, 2 * REC_VAL), f32),
            pltpu.VMEM((2, width, feats), bf16),
            pltpu.VMEM((2, deep, cols), bf16),
            pltpu.VMEM((rows, 2 * REC_KEY), f32),
            pltpu.VMEM((n, subs, nt, ROWS8, feats), bf16),
            pltpu.VMEM((seq, REC_KEY), f32),
            pltpu.VMEM((n, n, 8, rows), f32),
            pltpu.VMEM((rows, 128), f32),
            pltpu.VMEM((2, seq, width), f32),
            pltpu.VMEM((2, seq, width), bf16),
            pltpu.VMEM((2, seq, width), bf16),
            pltpu.VMEM((seq, width), bf16),
            pltpu.VMEM((REC_VAL, REC_KEY), f32),
            pltpu.VMEM((2, seq, wide), bf16),
            pltpu.VMEM((n, nt, piece, cols), bf16),
            pltpu.VMEM((n, nt, piece, cols), bf16),
            pltpu.VMEM((n, piece, cols), bf16),
            dma((19,)),
            dma((subs, nt)), dma((n, subs)), dma((subs,)),
            dma((n, subs, nt)), dma((n, subs, nt)), dma((2,)), dma((n,)), dma,
            dma((n, 2)), dma((n, n)), dma((2, chunks)), dma((2, chunks)),
            dma((nu, n)), dma((2, nu)), dma((n, nt)), dma((n, nt)), dma((n,)), dma((n,)), dma,
        ],
        compiler_params=pltpu.CompilerParams(collective_id=0, has_side_effects=True),
        name="layer",
    )(
        tokens.reshape(subs, nt, ROWS8, feats), norm_gain.reshape(1, -1), *args[2:8], decay_shift,
        args[8], args[9],
        score_offset, lower_bound.reshape(1, -1), rec_gain.reshape(1, -1),
    )


def on_device(*args):
    if stationary_fits(args):
        return stationary(*args)
    return gathered_plan(*args)


def solution(mesh):
    in_specs = (
        P(("grp", "sp"), "tp"),
        P(),
        P("tp", "sp"),
        P("tp", "sp"),
        P("tp", "sp"),
        P("tp", "sp"),
        P("tp", "sp"),
        P("tp", "sp"),
        P("tp", "sp"),
        P("tp", "sp"),
        P("tp"),
        P("tp"),
        P(("grp", "sp"), "tp"),
        P("tp"),
    )
    out_specs = P(("grp", "sp", "tp"), None)
    return jax.shard_map(
        on_device, mesh=mesh, in_specs=in_specs, out_specs=out_specs, check_vma=False
    )
```

```python
import contextlib
import functools

import jax
import jax.numpy as jnp
from jax import lax
from jax.experimental import pallas as pl
from jax.experimental.pallas import tpu as pltpu
from jax.sharding import PartitionSpec as P

HEAD = 64
REC_KEY = 128
REC_VAL = 128
SPAN = 64


EPS = 1e-06
TOP_PRECISION = lax.Precision.HIGHEST


def entering(x, axis, combine, identity):
    count, here = (lax.axis_size(axis), lax.axis_index(axis))
    everything = jax.tree.map(
        lambda part, kind: lax.all_gather(part.astype(kind), axis), x, (jnp.bfloat16, jnp.bfloat16)
    )
    start = jax.tree.map(
        lambda part, zero: jnp.broadcast_to(jnp.asarray(zero, part.dtype), part.shape), x, identity
    )

    def entering_turn(k, before):
        reached = k < here
        new = combine(
            before, jax.tree.map(lambda part, own: part[k].astype(own.dtype), everything, x)
        )
        return jax.tree.map(lambda a, b: jnp.where(reached, a, b), new, before)

    return lax.fori_loop(0, count, entering_turn, start)


def make_fold(norm_gain, weights, carry, piece):
    elementwise_sq, totals = carry
    raw = piece.astype(jnp.float32)
    scaled = (raw * norm_gain[None, :]).astype(jnp.bfloat16)
    elementwise_sq = jnp.sum(raw * raw, axis=1)
    updated = []
    for total, weight in zip(totals, weights):
        updated.append(
            lax.dot_general(
                scaled, weight, (((1,), (1,)), ((), ())), preferred_element_type=jnp.float32
            )
        )
    return (elementwise_sq, tuple(updated))


def project_all(tokens, norm_gain, weights):
    rows = tokens.shape[0]
    width = weights[0].shape[1]
    start_carry = (
        jnp.zeros((rows,), jnp.float32),
        tuple((jnp.zeros((rows, weight.shape[0]), jnp.float32) for weight in weights)),
    )
    elementwise_sq, totals = make_fold(
        norm_gain, weights, start_carry, lax.all_gather(tokens, "tp", axis=1, tiled=True)
    )
    inv_rms = lax.rsqrt(elementwise_sq / width + EPS)
    return tuple((total * inv_rms[:, None] for total in totals))


def attention(att_query, key_value, score_offset):
    rows = att_query.shape[0]
    gathered = lax.all_gather(key_value, "sp", axis=0, tiled=True)
    seq = gathered.shape[0]
    kv_heads = key_value.shape[1] // (2 * HEAD)
    q_heads = att_query.shape[1] // HEAD
    group = q_heads // kv_heads
    kv_width = kv_heads * HEAD
    queries = att_query.reshape(rows, kv_heads, group, HEAD)
    offsets = score_offset.reshape(kv_heads, group)
    kblock = min(1024, seq)
    first_row = lax.axis_index("sp") * rows
    query_pos = first_row + jnp.arange(rows, dtype=jnp.int32)
    count = (first_row + rows - 1) // kblock + 1

    def attention_turn(step, carry):
        summed, run = carry
        block_start = (count - 1 - step) * kblock
        block = lax.dynamic_slice_in_dim(gathered, block_start, kblock, 0)
        keys = block[:, :kv_width].reshape(kblock, kv_heads, HEAD)
        values = block[:, kv_width:].reshape(kblock, kv_heads, HEAD)
        score = (
            jnp.einsum("tkgd,skd->tkgs", queries, keys, preferred_element_type=jnp.float32)
            * HEAD ** (-0.5)
            + offsets[None, :, :, None]
        )
        key_pos = block_start + jnp.arange(kblock, dtype=jnp.int32)
        visible = (key_pos[None, :] < query_pos[:, None])[:, None, None, :]
        keep = jnp.where(visible, jax.nn.log_sigmoid(-score), 0.0)
        tail = lax.cumsum(keep, axis=3, reverse=True) - keep
        weight = jnp.where(
            visible, jnp.exp(jax.nn.log_sigmoid(score) + tail + run[..., None]), 0.0
        ).astype(jnp.bfloat16)
        summed = summed + jnp.einsum(
            "tkgs,skd->tkgd", weight, values, preferred_element_type=jnp.float32
        )
        return (summed, run + jnp.sum(keep, axis=3))

    start_carry = (
        jnp.zeros((rows, kv_heads, group, HEAD), jnp.float32),
        jnp.zeros((rows, kv_heads, group), jnp.float32),
    )
    summed, _ = lax.fori_loop(0, count, attention_turn, start_carry)
    return summed.reshape(rows, q_heads * HEAD).astype(jnp.bfloat16)


def block_pass(carry, inputs):
    state_matrix, prefix = carry
    query_rows, log_decay, keyed_values, value_rows = inputs
    span = query_rows.shape[0]
    cumulative_log = jnp.cumsum(log_decay, axis=0)
    lower = jnp.arange(span, dtype=jnp.int32)[:, None] >= jnp.arange(span, dtype=jnp.int32)[None, :]
    diff = cumulative_log[:, None] - cumulative_log[None, :]
    decay = jnp.exp(jnp.where(lower[:, :, None, None], diff, -jnp.inf))
    score = jnp.einsum(
        "thk,tshk,shk->ths", query_rows, decay, keyed_values, precision=TOP_PRECISION
    )
    inner = jnp.einsum("ths,shv->thv", score, value_rows, precision=TOP_PRECISION)
    outer_product = jnp.einsum(
        "ril,ilc->ric", query_rows * jnp.exp(cumulative_log), state_matrix, precision=TOP_PRECISION
    )
    final_state = cumulative_log[-1]
    state_matrix = state_matrix * jnp.exp(final_state)[:, :, None] + jnp.einsum(
        "iag,iax->agx",
        keyed_values * jnp.exp(final_state[None] - cumulative_log),
        value_rows,
        precision=TOP_PRECISION,
    )
    reach_limit = query_rows * jnp.exp(cumulative_log + prefix[None])
    return ((state_matrix, prefix + final_state), (inner + outer_product, reach_limit))


def chain(earlier, later):
    return (earlier[0] * later[0], earlier[1] * later[0][:, :, None] + later[1])


def recurrence(rec_query, rec_forget, rec_input, lower_bound, decay_shift, rec_gain):
    rows = rec_query.shape[0]
    heads = rec_gain.shape[0] // REC_VAL
    logit = rec_forget.astype(jnp.float32)
    gap = 1.0 - lower_bound
    log_decay = jnp.log(lower_bound + gap * jax.nn.sigmoid(logit)) + decay_shift
    keyed_values = gap * jax.nn.sigmoid(-logit)
    query_rows = jax.nn.silu(rec_query.astype(jnp.float32))
    blocks = rows // SPAN

    def split(array, depth):
        return array.reshape(blocks, SPAN, heads, depth)

    start_carry = (
        jnp.zeros((heads, REC_KEY, REC_VAL), jnp.float32),
        jnp.zeros((heads, REC_KEY), jnp.float32),
    )
    (state_matrix, total), (local, reach_limit) = lax.scan(
        block_pass,
        start_carry,
        (
            split(query_rows, REC_KEY),
            split(log_decay, REC_KEY),
            split(keyed_values, REC_KEY),
            split(rec_input.astype(jnp.float32), REC_VAL),
        ),
    )
    identity = (
        jnp.ones((heads, REC_KEY), jnp.float32),
        jnp.zeros((heads, REC_KEY, REC_VAL), jnp.float32),
    )
    incoming_state = entering((jnp.exp(total), state_matrix), "sp", chain, identity)
    running_memory = jnp.einsum(
        "lida,dao->lido", reach_limit, incoming_state[1], precision=TOP_PRECISION
    )
    rec_raw = (local + running_memory).reshape(rows, heads, REC_VAL)
    rescaled_input = (
        rec_raw
        * lax.rsqrt(jnp.mean(rec_raw * rec_raw, axis=2, keepdims=True) + EPS)
        * rec_gain.reshape(heads, REC_VAL)
    )
    return rescaled_input.reshape(rows, heads * REC_VAL).astype(jnp.bfloat16)


def gathered_plan(
    tokens,
    norm_gain,
    att_q_weight,
    att_k_weight,
    att_v_weight,
    rec_q_weight,
    rec_f_weight,
    rec_i_weight,
    att_out_weight,
    rec_out_weight,
    score_offset,
    lower_bound,
    decay_shift,
    rec_gain,
):
    inputs = (
        lax.all_gather(att_q_weight, "sp", axis=1, tiled=True),
        lax.all_gather(att_k_weight, "sp", axis=1, tiled=True),
        lax.all_gather(att_v_weight, "sp", axis=1, tiled=True),
        lax.all_gather(rec_q_weight, "sp", axis=1, tiled=True),
        lax.all_gather(rec_f_weight, "sp", axis=1, tiled=True),
        lax.all_gather(rec_i_weight, "sp", axis=1, tiled=True),
    )
    projected = project_all(tokens, norm_gain, inputs)
    att_query = projected[0].astype(jnp.bfloat16)
    key_value = jnp.concatenate(projected[1:3], axis=1).astype(jnp.bfloat16)
    rec_query = projected[3].astype(jnp.bfloat16)
    rec_forget = projected[4].astype(jnp.bfloat16)
    rec_input = projected[5].astype(jnp.bfloat16)
    att_out = attention(att_query, key_value, score_offset)
    rec_out = recurrence(rec_query, rec_forget, rec_input, lower_bound, decay_shift, rec_gain)
    outputs = (
        lax.all_gather(att_out_weight, "sp", axis=1, tiled=True),
        lax.all_gather(rec_out_weight, "sp", axis=1, tiled=True),
    )
    att_rows, rec_rows = outputs
    return lax.psum_scatter(
        (
            jnp.dot(att_out, att_rows, preferred_element_type=jnp.float32)
            + jnp.dot(rec_out, rec_rows, preferred_element_type=jnp.float32)
        ).astype(jnp.bfloat16),
        "tp",
        scatter_dimension=0,
        tiled=True,
    )


MESH = pl.DeviceIdType.MESH
STEP = 32


def dot_nt(a, b):
    return lax.dot_general(a, b, (((1,), (1,)), ((), ())), preferred_element_type=jnp.float32)


def dot_tn(a, b):
    return lax.dot_general(a, b, (((0,), (0,)), ((), ())), preferred_element_type=jnp.float32)


def dot_nn(a, b):
    return jnp.dot(a, b, preferred_element_type=jnp.float32)


def remote(src, dst, send_sem, recv_sem, target):
    return pltpu.make_async_remote_copy(
        src_ref=src,
        dst_ref=dst,
        send_sem=send_sem,
        recv_sem=recv_sem,
        device_id=target,
        device_id_type=MESH,
    )


SUB = 32
ROWS8 = 8
LAST = 64
PROFILE = False


def scope(name):
    return jax.named_scope(name) if PROFILE else contextlib.nullcontext()


def stick_block(first, rows, j, group, x, offset_ref):
    block = 128
    q, base = first // block, first % block
    low = lax.broadcasted_iota(jnp.int32, (block, block), 0)
    high = lax.broadcasted_iota(jnp.int32, (block, block), 1)
    later = (low > high).astype(jnp.bfloat16)
    row = lax.broadcasted_iota(jnp.int32, (rows, block), 0) + base
    col = lax.broadcasted_iota(jnp.int32, (rows, block), 1)
    visible = jnp.concatenate([col < row] * group, axis=0)
    offset = jnp.concatenate(
        [jnp.full((rows, block), offset_ref[j * group + g], jnp.float32) for g in range(group)],
        axis=0,
    )
    queries = x[first:first + rows, :group * HEAD]
    queries = jnp.concatenate([queries[:, g * HEAD:(g + 1) * HEAD] for g in range(group)], axis=0)
    run = jnp.zeros((group * rows, 1), jnp.float32)
    summed = jnp.zeros((group * rows, HEAD), jnp.float32)
    for c in range(q, -1, -1):
        keys = x[c * block:(c + 1) * block, group * HEAD:(group + 1) * HEAD]
        values = x[c * block:(c + 1) * block, (group + 1) * HEAD:(group + 2) * HEAD]
        score = dot_nt(queries, keys) * HEAD ** (-0.5) + offset
        keep = -(jnp.maximum(score, 0.0) + jnp.log1p(jnp.exp(-jnp.abs(score))))
        gate = score + keep
        if c == q:
            keep = jnp.where(visible, keep, 0.0)
        top = keep.astype(jnp.bfloat16)
        rest = (keep - top.astype(jnp.float32)).astype(jnp.bfloat16)
        tail = dot_nn(top, later) + dot_nn(rest, later)
        weight = jnp.exp(gate + tail + run)
        if c == q:
            weight = jnp.where(visible, weight, 0.0)
        summed = summed + dot_nn(weight.astype(jnp.bfloat16), values)
        run = run + jnp.sum(keep, axis=1, keepdims=True)
    return jnp.concatenate(
        [summed[g * rows:(g + 1) * rows] for g in range(group)], axis=1
    ).astype(jnp.bfloat16)


def state_block(begin, rows, x, first, bound, gain, shift_ref, state_ref):
    gap = 1.0 - bound
    low = lax.broadcasted_iota(jnp.int32, (rows, rows), 0)
    high = lax.broadcasted_iota(jnp.int32, (rows, rows), 1)
    upto = ((high <= low) & (high // STEP == low // STEP)).astype(jnp.float32)
    lower = (
        lax.broadcasted_iota(jnp.int32, (STEP, STEP), 0)
        >= lax.broadcasted_iota(jnp.int32, (STEP, STEP), 1)
    )
    state = jnp.zeros((REC_VAL, REC_KEY), jnp.float32) if begin == 0 else state_ref[...]
    at = slice(begin, begin + rows)
    query = x[at, first:first + REC_KEY].astype(jnp.float32)
    logit = x[at, first + REC_KEY:first + 2 * REC_KEY].astype(jnp.float32)
    value = x[at, first + 2 * REC_KEY:first + 2 * REC_KEY + REC_VAL]
    log_decay = jnp.log(bound + gap * jax.nn.sigmoid(logit)) + shift_ref[at].astype(jnp.float32)
    keyed = gap * jax.nn.sigmoid(-logit)
    query = query * jax.nn.sigmoid(query)
    running = jnp.dot(upto, log_decay, precision=TOP_PRECISION, preferred_element_type=jnp.float32)
    outs = []
    for i in range(rows // STEP):
        it = slice(i * STEP, (i + 1) * STEP)
        cumulative, q, k, v = running[it], query[it], keyed[it], value[it]
        middle = cumulative[STEP // 2 - 1:STEP // 2]
        last = cumulative[STEP - 1:STEP]
        score = dot_nt(
            (q * jnp.exp(cumulative - middle)).astype(jnp.bfloat16),
            (k * jnp.exp(middle - cumulative)).astype(jnp.bfloat16),
        )
        score = jnp.where(lower, score, 0.0).astype(jnp.bfloat16)
        raw = dot_nn(score, v) + dot_nt(
            (q * jnp.exp(cumulative)).astype(jnp.bfloat16), state.astype(jnp.bfloat16)
        )
        state = state * jnp.exp(last) + dot_tn(
            v, (k * jnp.exp(last - cumulative)).astype(jnp.bfloat16)
        )
        scale = lax.rsqrt(jnp.mean(raw * raw, axis=1, keepdims=True) + EPS)
        outs.append((raw * scale * gain).astype(jnp.bfloat16))
    state_ref[...] = state
    return jnp.concatenate(outs, axis=0)


def units_of(n, rows):
    whole = [(k * rows, rows) for k in range(n - 1)]
    return whole + [((n - 1) * rows + r, LAST) for r in range(0, rows, LAST)]


def layer_kernel(
    n, nt, group,
    tok_ref, gain_ref, aq_ref, ak_ref, av_ref, rq_ref, rf_ref, ri_ref, shift_ref,
    wa_ref, wr_ref, offset_ref, bound_ref, rec_gain_ref,
    out_ref,
    tokens, gains, bounds, rec_gains, weights, outs, wide_shift, own_shift, tbuf, shifts, squares, scales,
    part, sent, came, x, state, heads, shares, landed, mixed,
    l_sem, a_send, a_recv, b_send, b_recv, d_send, d_recv, q_send, q_recv,
    c_send, c_recv, e_send, e_recv, f_send, f_recv, g_send, g_recv,
):
    s, t = lax.axis_index("sp"), lax.axis_index("tp")
    rows, feats = own_shift.shape[0], tokens.shape[-1]
    piece = rows // nt
    width = x.shape[1]
    att_width = (group + 2) * HEAD
    wide = group * HEAD
    cols = outs.shape[-1]
    subs = rows // SUB
    ends = (0, n - 1)
    f32, bf16 = jnp.float32, jnp.bfloat16
    units = units_of(n, rows)
    nu = len(units)

    load_tokens = pltpu.make_async_copy(tok_ref, tokens, l_sem.at[0])
    load_gain = pltpu.make_async_copy(
        gain_ref.at[:, pl.ds(pl.multiple_of(s * feats, feats), feats)], gains, l_sem.at[1]
    )
    load_weights = []
    first = 0
    for ref, size in (
        (aq_ref, wide), (ak_ref, HEAD), (av_ref, HEAD),
        (rq_ref, REC_KEY), (rf_ref, REC_KEY), (ri_ref, REC_VAL),
    ):
        for i in range(2):
            load_weights.append(
                pltpu.make_async_copy(
                    ref.at[pl.ds(i * size, size)], weights.at[i, pl.ds(first, size)], l_sem.at[2]
                )
            )
        first += size
    load_shift = pltpu.make_async_copy(shift_ref, wide_shift, l_sem.at[3])
    load_bounds = pltpu.make_async_copy(bound_ref, bounds, l_sem.at[4])
    load_rec_gains = pltpu.make_async_copy(rec_gain_ref, rec_gains, l_sem.at[5])
    load_outs = [
        pltpu.make_async_copy(ref, outs.at[o], l_sem.at[6]) for o, ref in enumerate((wa_ref, wr_ref))
    ]

    load_tokens.start()
    barrier = pltpu.get_barrier_semaphore()
    for a in range(n):
        for b in range(nt):
            if a or b:
                pl.semaphore_signal(
                    barrier, inc=1,
                    device_id={"sp": lax.rem(s + a, n), "tp": lax.rem(t + b, nt)},
                    device_id_type=MESH,
                )
    for load in (
        load_shift, load_gain, *load_weights, load_bounds, load_rec_gains, *load_outs
    ):
        load.start()
    load_tokens.wait()
    with scope("barrier"):
        pl.semaphore_wait(barrier, n * nt - 1)

    def plane(v):
        others = [i for i in range(2) if v != ends[i]]
        mine = [i for i in range(2) if v == ends[i]]
        order = (1, 0) if v < n // 2 else (0, 1)

        def parts_of(k):
            return range(subs) if k == 0 else (slice(None),)

        def slot(c):
            return 0 if isinstance(c, slice) else c

        def lane_of(k, c):
            return c if k == 0 else subs + k - 1

        def first_copy(c, j):
            return remote(
                tokens.at[c, j], tbuf.at[v, c, j], a_send, a_recv.at[lane_of(v, c)],
                {"sp": t, "tp": j},
            )

        def first_here(c):
            return pltpu.make_async_copy(
                tokens.at[c, v], tbuf.at[v, c, v], a_recv.at[lane_of(v, c)]
            )

        def send_first(when):
            pl.when(when)(send_first_now)

        def send_first_now():
            for c in parts_of(v):
                for j in range(nt):
                    if j == v:
                        pl.when(t != v)(lambda: first_copy(c, j).start())
                        pl.when(t == v)(lambda: first_here(c).start())
                    else:
                        first_copy(c, j).start()

        def second_copy(k, c, d):
            return remote(
                tbuf.at[k, c, t], tbuf.at[k, c, t],
                b_send, b_recv.at[lane_of(k, c)],
                {"tp": lax.rem(t + d, nt)},
            )

        def relay(k, c):
            with scope(f"relay{k}"):
                remote(
                    tokens.at[c, 0], tbuf.at[k, c, t], a_send, a_recv.at[lane_of(k, c)],
                    {"sp": (v + 1) % n},
                ).wait_recv()
            for d in range(1, nt):
                second_copy(k, c, d).start()

        def square_copy(k, i):
            return remote(
                squares.at[v, k], squares.at[v, k], q_send.at[i], q_recv.at[k],
                {"sp": ends[i]},
            )

        def chain_copy(i, c):
            to = v - 1 if i == 0 else v + 1
            return remote(
                sent.at[i, pl.ds(c * SUB, SUB)], came.at[i, pl.ds(c * SUB, SUB)],
                c_send.at[i], c_recv.at[i, c], {"sp": to},
            )

        def project(k, c):
            with scope(f"wtok{k}"):
                most = tbuf.at[k, c, pl.ds(0, nt - 1)]
                remote(
                    most, most, b_send, b_recv.at[lane_of(k, c)], {"tp": lax.rem(t + 1, nt)}
                ).wait_recv()
            size = rows if isinstance(c, slice) else SUB
            begin = k * rows + slot(c) * SUB
            raw = tbuf[k, c].reshape(size, feats).astype(f32)
            scaled = (raw * gains[...]).astype(bf16)
            for i in order:
                product = dot_nt(scaled, weights[i])
                if v == ends[1 - i]:
                    for r in range(size // SUB):
                        at = begin + r * SUB
                        sent[i, pl.ds(at, SUB)] = product[r * SUB:(r + 1) * SUB].astype(bf16)
                        chain_copy(i, at // SUB).start()
                else:
                    part[i, pl.ds(begin, size)] = product

        def square(k):
            raw = tbuf[k].reshape(rows, feats).astype(f32)
            total = jnp.sum(raw * raw, axis=1, keepdims=True)
            flat = jnp.transpose(jnp.broadcast_to(total, (rows, 128)))
            squares[v, k] = flat[:8]
            for i in others:
                square_copy(k, i).start()

        def shift_copy(i):
            return remote(
                own_shift.at[:, pl.ds(i * REC_KEY, REC_KEY)], shifts.at[pl.ds(v * rows, rows)],
                d_send.at[i], d_recv.at[v], {"sp": ends[i]},
            )

        def shift_here(i):
            return pltpu.make_async_copy(
                own_shift.at[:, pl.ds(i * REC_KEY, REC_KEY)], shifts.at[pl.ds(v * rows, rows)],
                d_recv.at[v],
            )

        def send_shift(i):
            if v == ends[i]:
                shift_here(i).start()
            else:
                shift_copy(i).start()

        def forward(i, c):
            with scope(f"chain{i}_{c}"):
                chain_copy(i, c).wait_recv()
            at = (i, pl.ds(c * SUB, SUB))
            sent[at] = (part[at] + came[at].astype(f32)).astype(bf16)
            chain_copy(i, c).start()

        def head_copy(i, u, to):
            at = (i, pl.ds(units[u][0], units[u][1]))
            return remote(
                heads.at[at], heads.at[at], e_send.at[to], e_recv.at[i, u], {"sp": to}
            )

        def near(i):
            return 1 if i == 0 else n - 2

        def between(i):
            return [p for p in range(1, n - 1) if p != near(i)]

        def direct(u):
            return units[u][1] == LAST

        def relayed(i, u):
            return u == 0 or (u == 1 and i == 1)

        def head_targets(i, u):
            far = ends[1 - i]
            if relayed(i, u):
                return [] if v == far else [v + 1 if i == 0 else v - 1]
            if v == ends[i]:
                if direct(u):
                    return [far, *between(i), near(i)]
                return [near(i), far]
            if v == near(i) and not direct(u):
                return between(i)
            return []

        def send_heads(i, u, to):
            head_copy(i, u, to).start()

        def wait_heads(i, u):
            with scope(f"whead{i}_{u}"):
                head_copy(i, u, ends[i]).wait_recv()

        def mix(u):
            e = mine[0]
            begin, size = units[u]
            k = begin // rows
            span = pl.ds(begin, size)
            with scope(f"wmix{u}"):
                for c in range(begin // SUB, (begin + size) // SUB):
                    chain_copy(e, c).wait_recv()
            if begin % rows == 0:
                most = squares.at[pl.ds(0, n - 1), k]
                remote(most, most, q_send.at[e], q_recv.at[k], {"sp": ends[1 - e]}).wait_recv()
                remote(
                    own_shift.at[:, pl.ds(e * REC_KEY, REC_KEY)],
                    shifts.at[pl.ds(k * rows, rows)], d_send.at[e], d_recv.at[k],
                    {"sp": ends[1 - e]},
                ).wait_recv()
                total = squares[0, k, :1]
                for p in range(1, n):
                    total = total + squares[p, k, :1]
                inv_rms = lax.rsqrt(total / (feats * n) + EPS)
                scales[...] = jnp.transpose(jnp.broadcast_to(inv_rms, (128, rows)))
            inv_rms = scales[pl.ds(begin % rows, size)]
            for c in range(width // 128):
                lane = pl.ds(c * 128, 128)
                result = part[e, span, lane] + came[e, span, lane].astype(f32)
                x[span, lane] = (result * inv_rms).astype(bf16)
            with scope(f"stick{u}"):
                heads[e, span, pl.ds(0, wide)] = stick_block(
                    begin, size, e, group, x, offset_ref
                )
            with scope(f"state{u}"):
                heads[e, span, pl.ds(wide, REC_VAL)] = state_block(
                    begin, size, x, att_width,
                    bounds[:, pl.ds(e * REC_KEY, REC_KEY)],
                    rec_gains[:, pl.ds(e * REC_VAL, REC_VAL)], shifts, state,
                )

        def share_copy(k, b):
            to = lax.rem(t + b, nt)
            return remote(
                shares.at[k, to], landed.at[k, b], f_send, f_recv.at[k], {"tp": to}
            )

        def multiply(u):
            begin, size = units[u]
            k = begin // rows
            span = pl.ds(begin, size)
            total = None
            for i in range(2):
                for o, at, deep in ((0, 0, wide), (1, wide, REC_VAL)):
                    term = dot_nn(heads[i, span, pl.ds(at, deep)], outs[o, pl.ds(i * deep, deep)])
                    total = term if total is None else total + term
            total = total.astype(bf16)
            if size == rows:
                shares[k] = total.reshape(nt, piece, cols)
                for b in range(1, nt):
                    share_copy(k, b).start()
            else:
                for j in range(begin % rows // piece, (begin % rows + size) // piece):
                    at = j * piece - begin % rows
                    shares[k, j] = total[at:at + piece]
                    b = lax.rem(j - t + nt, nt)
                    pl.when(t != j)(lambda: share_copy(k, b).start())

        place = out_ref.at[:, pl.ds(v * cols, cols)]

        def final_copy(k):
            return remote(mixed.at[k], place, g_send, g_recv, {"sp": k})

        def final_here():
            return pltpu.make_async_copy(mixed.at[v], place, g_recv)

        def combine(k):
            with scope(f"wshare{k}"):
                most = pl.ds(1, nt - 1)
                remote(
                    shares.at[k, most], landed.at[k, most], f_send, f_recv.at[k],
                    {"tp": lax.rem(t + 1, nt)},
                ).wait_recv()
            result = shares[k, t].astype(f32)
            for b in range(1, nt):
                result = result + landed[k, b].astype(f32)
            mixed[k] = result.astype(bf16)
            if k == v:
                final_here().start()
            else:
                final_copy(k).start()

        def projection_loaded():
            load_gain.wait()
            pltpu.make_async_copy(weights, weights, l_sem.at[2]).wait()

        def rest_loaded():
            load_bounds.wait()
            load_rec_gains.wait()
            pltpu.make_async_copy(outs, outs, l_sem.at[6]).wait()

        events = []

        def event(time, *call):
            events.append((time, len(events), call))

        starts = (START0, START1)
        hops = (n - 1 - v, v)
        whole = slice(None)
        event(5.9, projection_loaded)
        def round_shift():
            own_shift[...] = wide_shift[...].astype(bf16)

        event(0.1, load_shift.wait)
        event(0.15, round_shift)
        event(15.0, rest_loaded)
        soon = t < v
        if v < n // 2:
            soon = soon | (t == n - 1)
        if v == 0:
            soon = t >= 0
        event(0.0, send_first, soon)
        for c in range(subs):
            event(4.0 + 0.1 * c, relay, 0, c)
        event(4.05, send_first, jnp.logical_not(soon))
        for c in range(subs):
            event(6.0 + 0.1 * c, project, 0, c)
        event(0.2, send_shift, 0)
        event(4.4 if 0 < v < n - 1 else 0.2, send_shift, 1)
        event(7.1, square, 0)
        ready = [6.5]
        for k in range(1, n):
            event(6.05 if k == 1 else 9.0 + 0.1 * k, relay, k, whole)
            at = (TOKENS if v in ends else TOKENS_MID)[k - 1]
            event(at, project, k, whole)
            event(at + 0.1, square, k)
            ready.append(at + 0.01)
        chain_end = 0.0
        if v not in ends:
            for i in range(2):
                for c in range(n * subs):
                    at = max(starts[i] + hops[i] * HOP + CHUNK * c, ready[c // subs])
                    event(at, forward, i, c)
                    chain_end = max(chain_end, at)
        done = [[0.0] * nu, [0.0] * nu]
        for i in range(2):
            at = 0.0
            for u, (begin, size) in enumerate(units):
                last = (begin + size) // SUB - 1
                arrive = max(at, starts[i] + (n - 1) * HOP + CHUNK * last)
                at = arrive + (1.8 if size == rows else 1.6)
                done[i][u] = at
                if v == ends[i]:
                    event(arrive, mix, u)
                    for to in head_targets(i, u):
                        event(at - 0.1, send_heads, i, u, to)
        for u, (begin, size) in enumerate(units):
            k = begin // rows
            latest = max(done[0][u], done[1][u])
            for i in others:
                away = v if i == 0 else n - 1 - v
                if direct(u):
                    at = done[i][u] + 5.0
                elif relayed(i, u):
                    at = done[i][u] + 4.2 * away
                elif v == near(i):
                    at = done[i][u] + 4.2
                elif v == ends[1 - i]:
                    at = done[i][u] + 6.5
                else:
                    at = done[i][u] + 8.4
                latest = max(latest, chain_end)
                if v != near(i):
                    at = max(at, chain_end)
                event(at, wait_heads, i, u)
                for to in head_targets(i, u):
                    event(at, send_heads, i, u, to)
                latest = max(latest, at)
            event(latest + 0.1, multiply, u)
            if begin + size == (k + 1) * rows:
                event(latest + 4.0, combine, k)
        for _, _, (call, *args) in sorted(events, key=lambda e: e[:2]):
            call(*args)

        with scope("wfinal"):
            pltpu.make_async_copy(out_ref, out_ref, g_recv).wait()

        with scope("wsend"):
            def sent_all(src, sem):
                remote(src, src, sem, a_recv.at[0], {"sp": (v + 1) % n}).wait_send()

            pl.when(t != v)(lambda: sent_all(tokens, a_send))
            pl.when(t == v)(lambda: sent_all(tokens.at[:, pl.ds(0, nt - 1)], a_send))
            sent_all(tbuf.at[:, :, pl.ds(0, nt - 1)], b_send)
            sent_all(shares.at[:, pl.ds(0, nt - 1)], f_send)
            sent_all(mixed.at[pl.ds(0, n - 1)], g_send)
            for i in others:
                sent_all(own_shift.at[:, pl.ds(i * REC_KEY, REC_KEY)], d_send.at[i])
                sent_all(squares.at[v], q_send.at[i])
                sent_all(sent.at[i], c_send.at[i])
            for to in range(n):
                spans = [
                    units[u] for i in range(2) for u in range(nu) if to in head_targets(i, u)
                ]
                if spans:
                    begin = spans[0][0]
                    size = sum(size for _, size in spans)
                    sent_all(heads.at[0, pl.ds(begin, size)], e_send.at[to])

    for v in range(n):
        if v in ends:
            @pl.when(s == v)
            def _():
                x[pl.ds((n - 1) * rows, rows)] = jnp.zeros((rows, width), bf16)
                plane(v)
        else:
            pl.when(s == v)(functools.partial(plane, v))


START0, START1, HOP, CHUNK = 8.0, 6.3, 3.6, 0.88
TOKENS = (10.5, 11.5, 12.5)
TOKENS_MID = (10.5, 14.0, 16.5)


def stationary_fits(args):
    n, nt = lax.axis_size("sp"), lax.axis_size("tp")
    tokens, att_q, att_k, rec_i = args[0], args[2], args[3], args[7]
    rows, feats = tokens.shape
    return (
        n == nt
        and n >= 3
        and att_k.shape[0] // HEAD == 2
        and rec_i.shape[0] // REC_VAL == 2
        and (att_q.shape[0] // att_k.shape[0]) * HEAD == 128
        and feats == att_q.shape[1]
        and rows == 128
        and rows == SUB * nt
        and SUB == ROWS8 * nt
    )


def stationary(*args):
    n, nt = lax.axis_size("sp"), lax.axis_size("tp")
    tokens, norm_gain, att_q, att_k = args[:4]
    score_offset, lower_bound, decay_shift, rec_gain = args[10:]
    rows, feats = tokens.shape
    seq = rows * n
    deep, cols = args[8].shape
    group = att_q.shape[0] // att_k.shape[0]
    width = (group + 2) * HEAD + 2 * REC_KEY + REC_VAL
    wide = group * HEAD + REC_VAL
    piece = rows // nt
    chunks = seq // SUB
    subs = rows // SUB
    nu = len(units_of(n, rows))
    bf16, f32 = jnp.bfloat16, jnp.float32
    dma = pltpu.SemaphoreType.DMA
    vmem = pl.BlockSpec(memory_space=pltpu.VMEM)
    hbm = pl.BlockSpec(memory_space=pl.ANY)
    smem = pl.BlockSpec(memory_space=pltpu.SMEM)
    return pl.pallas_call(
        functools.partial(layer_kernel, n, nt, group),
        out_shape=jax.ShapeDtypeStruct((piece, cols * n), bf16),
        in_specs=[hbm] * 11 + [smem, hbm, hbm],
        out_specs=hbm,
        scratch_shapes=[
            pltpu.VMEM((subs, nt, ROWS8, feats), bf16),
            pltpu.VMEM((1, feats), f32),
            pltpu.VMEM((1, 2 * REC_KEY), f32),
            pltpu.VMEM((1, 2 * REC_VAL), f32),
            pltpu.VMEM((2, width, feats), bf16),
            pltpu.VMEM((2, deep, cols), bf16),
            pltpu.VMEM((rows, 2 * REC_KEY), f32),
            pltpu.VMEM((rows, 2 * REC_KEY), bf16),
            pltpu.VMEM((n, subs, nt, ROWS8, feats), bf16),
            pltpu.VMEM((seq, REC_KEY), bf16),
            pltpu.VMEM((n, n, 8, rows), f32),
            pltpu.VMEM((rows, 128), f32),
            pltpu.VMEM((2, seq, width), f32),
            pltpu.VMEM((2, seq, width), bf16),
            pltpu.VMEM((2, seq, width), bf16),
            pltpu.VMEM((seq, width), bf16),
            pltpu.VMEM((REC_VAL, REC_KEY), f32),
            pltpu.VMEM((2, seq, wide), bf16),
            pltpu.VMEM((n, nt, piece, cols), bf16),
            pltpu.VMEM((n, nt, piece, cols), bf16),
            pltpu.VMEM((n, piece, cols), bf16),
            dma((7,)), dma, dma((subs + n - 1,)), dma, dma((subs + n - 1,)), dma((2,)), dma((n,)),
            dma((2,)), dma((n,)), dma((2,)), dma((2, chunks)), dma((n,)), dma((2, nu)),
            dma, dma((n,)), dma, dma,
        ],
        compiler_params=pltpu.CompilerParams(collective_id=0, has_side_effects=True),
        name="layer",
    )(
        tokens.reshape(subs, nt, ROWS8, feats), norm_gain.reshape(1, -1), *args[2:8], decay_shift,
        args[8], args[9],
        score_offset, lower_bound.reshape(1, -1), rec_gain.reshape(1, -1),
    )


def on_device(*args):
    if stationary_fits(args):
        return stationary(*args)
    return gathered_plan(*args)


def solution(mesh):
    in_specs = (
        P(("grp", "sp"), "tp"),
        P(),
        P("tp", "sp"),
        P("tp", "sp"),
        P("tp", "sp"),
        P("tp", "sp"),
        P("tp", "sp"),
        P("tp", "sp"),
        P("tp", "sp"),
        P("tp", "sp"),
        P("tp"),
        P("tp"),
        P(("grp", "sp"), "tp"),
        P("tp"),
    )
    out_specs = P(("grp", "sp", "tp"), None)
    return jax.shard_map(
        on_device, mesh=mesh, in_specs=in_specs, out_specs=out_specs, check_vma=False
    )
```

```python
import contextlib
import functools

import jax
import jax.numpy as jnp
from jax import lax
from jax.experimental import pallas as pl
from jax.experimental.pallas import tpu as pltpu
from jax.sharding import PartitionSpec as P

HEAD = 64
REC_KEY = 128
REC_VAL = 128
SPAN = 64


EPS = 1e-06
TOP_PRECISION = lax.Precision.HIGHEST


def entering(x, axis, combine, identity):
    count, here = (lax.axis_size(axis), lax.axis_index(axis))
    everything = jax.tree.map(
        lambda part, kind: lax.all_gather(part.astype(kind), axis), x, (jnp.bfloat16, jnp.bfloat16)
    )
    start = jax.tree.map(
        lambda part, zero: jnp.broadcast_to(jnp.asarray(zero, part.dtype), part.shape), x, identity
    )

    def entering_turn(k, before):
        reached = k < here
        new = combine(
            before, jax.tree.map(lambda part, own: part[k].astype(own.dtype), everything, x)
        )
        return jax.tree.map(lambda a, b: jnp.where(reached, a, b), new, before)

    return lax.fori_loop(0, count, entering_turn, start)


def make_fold(norm_gain, weights, carry, piece):
    elementwise_sq, totals = carry
    raw = piece.astype(jnp.float32)
    scaled = (raw * norm_gain[None, :]).astype(jnp.bfloat16)
    elementwise_sq = jnp.sum(raw * raw, axis=1)
    updated = []
    for total, weight in zip(totals, weights):
        updated.append(
            lax.dot_general(
                scaled, weight, (((1,), (1,)), ((), ())), preferred_element_type=jnp.float32
            )
        )
    return (elementwise_sq, tuple(updated))


def project_all(tokens, norm_gain, weights):
    rows = tokens.shape[0]
    width = weights[0].shape[1]
    start_carry = (
        jnp.zeros((rows,), jnp.float32),
        tuple((jnp.zeros((rows, weight.shape[0]), jnp.float32) for weight in weights)),
    )
    elementwise_sq, totals = make_fold(
        norm_gain, weights, start_carry, lax.all_gather(tokens, "tp", axis=1, tiled=True)
    )
    inv_rms = lax.rsqrt(elementwise_sq / width + EPS)
    return tuple((total * inv_rms[:, None] for total in totals))


def attention(att_query, key_value, score_offset):
    rows = att_query.shape[0]
    gathered = lax.all_gather(key_value, "sp", axis=0, tiled=True)
    seq = gathered.shape[0]
    kv_heads = key_value.shape[1] // (2 * HEAD)
    q_heads = att_query.shape[1] // HEAD
    group = q_heads // kv_heads
    kv_width = kv_heads * HEAD
    queries = att_query.reshape(rows, kv_heads, group, HEAD)
    offsets = score_offset.reshape(kv_heads, group)
    kblock = min(1024, seq)
    first_row = lax.axis_index("sp") * rows
    query_pos = first_row + jnp.arange(rows, dtype=jnp.int32)
    count = (first_row + rows - 1) // kblock + 1

    def attention_turn(step, carry):
        summed, run = carry
        block_start = (count - 1 - step) * kblock
        block = lax.dynamic_slice_in_dim(gathered, block_start, kblock, 0)
        keys = block[:, :kv_width].reshape(kblock, kv_heads, HEAD)
        values = block[:, kv_width:].reshape(kblock, kv_heads, HEAD)
        score = (
            jnp.einsum("tkgd,skd->tkgs", queries, keys, preferred_element_type=jnp.float32)
            * HEAD ** (-0.5)
            + offsets[None, :, :, None]
        )
        key_pos = block_start + jnp.arange(kblock, dtype=jnp.int32)
        visible = (key_pos[None, :] < query_pos[:, None])[:, None, None, :]
        keep = jnp.where(visible, jax.nn.log_sigmoid(-score), 0.0)
        tail = lax.cumsum(keep, axis=3, reverse=True) - keep
        weight = jnp.where(
            visible, jnp.exp(jax.nn.log_sigmoid(score) + tail + run[..., None]), 0.0
        ).astype(jnp.bfloat16)
        summed = summed + jnp.einsum(
            "tkgs,skd->tkgd", weight, values, preferred_element_type=jnp.float32
        )
        return (summed, run + jnp.sum(keep, axis=3))

    start_carry = (
        jnp.zeros((rows, kv_heads, group, HEAD), jnp.float32),
        jnp.zeros((rows, kv_heads, group), jnp.float32),
    )
    summed, _ = lax.fori_loop(0, count, attention_turn, start_carry)
    return summed.reshape(rows, q_heads * HEAD).astype(jnp.bfloat16)


def block_pass(carry, inputs):
    state_matrix, prefix = carry
    query_rows, log_decay, keyed_values, value_rows = inputs
    span = query_rows.shape[0]
    cumulative_log = jnp.cumsum(log_decay, axis=0)
    lower = jnp.arange(span, dtype=jnp.int32)[:, None] >= jnp.arange(span, dtype=jnp.int32)[None, :]
    diff = cumulative_log[:, None] - cumulative_log[None, :]
    decay = jnp.exp(jnp.where(lower[:, :, None, None], diff, -jnp.inf))
    score = jnp.einsum(
        "thk,tshk,shk->ths", query_rows, decay, keyed_values, precision=TOP_PRECISION
    )
    inner = jnp.einsum("ths,shv->thv", score, value_rows, precision=TOP_PRECISION)
    outer_product = jnp.einsum(
        "ril,ilc->ric", query_rows * jnp.exp(cumulative_log), state_matrix, precision=TOP_PRECISION
    )
    final_state = cumulative_log[-1]
    state_matrix = state_matrix * jnp.exp(final_state)[:, :, None] + jnp.einsum(
        "iag,iax->agx",
        keyed_values * jnp.exp(final_state[None] - cumulative_log),
        value_rows,
        precision=TOP_PRECISION,
    )
    reach_limit = query_rows * jnp.exp(cumulative_log + prefix[None])
    return ((state_matrix, prefix + final_state), (inner + outer_product, reach_limit))


def chain(earlier, later):
    return (earlier[0] * later[0], earlier[1] * later[0][:, :, None] + later[1])


def recurrence(rec_query, rec_forget, rec_input, lower_bound, decay_shift, rec_gain):
    rows = rec_query.shape[0]
    heads = rec_gain.shape[0] // REC_VAL
    logit = rec_forget.astype(jnp.float32)
    gap = 1.0 - lower_bound
    log_decay = jnp.log(lower_bound + gap * jax.nn.sigmoid(logit)) + decay_shift
    keyed_values = gap * jax.nn.sigmoid(-logit)
    query_rows = jax.nn.silu(rec_query.astype(jnp.float32))
    blocks = rows // SPAN

    def split(array, depth):
        return array.reshape(blocks, SPAN, heads, depth)

    start_carry = (
        jnp.zeros((heads, REC_KEY, REC_VAL), jnp.float32),
        jnp.zeros((heads, REC_KEY), jnp.float32),
    )
    (state_matrix, total), (local, reach_limit) = lax.scan(
        block_pass,
        start_carry,
        (
            split(query_rows, REC_KEY),
            split(log_decay, REC_KEY),
            split(keyed_values, REC_KEY),
            split(rec_input.astype(jnp.float32), REC_VAL),
        ),
    )
    identity = (
        jnp.ones((heads, REC_KEY), jnp.float32),
        jnp.zeros((heads, REC_KEY, REC_VAL), jnp.float32),
    )
    incoming_state = entering((jnp.exp(total), state_matrix), "sp", chain, identity)
    running_memory = jnp.einsum(
        "lida,dao->lido", reach_limit, incoming_state[1], precision=TOP_PRECISION
    )
    rec_raw = (local + running_memory).reshape(rows, heads, REC_VAL)
    rescaled_input = (
        rec_raw
        * lax.rsqrt(jnp.mean(rec_raw * rec_raw, axis=2, keepdims=True) + EPS)
        * rec_gain.reshape(heads, REC_VAL)
    )
    return rescaled_input.reshape(rows, heads * REC_VAL).astype(jnp.bfloat16)


def gathered_plan(
    tokens,
    norm_gain,
    att_q_weight,
    att_k_weight,
    att_v_weight,
    rec_q_weight,
    rec_f_weight,
    rec_i_weight,
    att_out_weight,
    rec_out_weight,
    score_offset,
    lower_bound,
    decay_shift,
    rec_gain,
):
    inputs = (
        lax.all_gather(att_q_weight, "sp", axis=1, tiled=True),
        lax.all_gather(att_k_weight, "sp", axis=1, tiled=True),
        lax.all_gather(att_v_weight, "sp", axis=1, tiled=True),
        lax.all_gather(rec_q_weight, "sp", axis=1, tiled=True),
        lax.all_gather(rec_f_weight, "sp", axis=1, tiled=True),
        lax.all_gather(rec_i_weight, "sp", axis=1, tiled=True),
    )
    projected = project_all(tokens, norm_gain, inputs)
    att_query = projected[0].astype(jnp.bfloat16)
    key_value = jnp.concatenate(projected[1:3], axis=1).astype(jnp.bfloat16)
    rec_query = projected[3].astype(jnp.bfloat16)
    rec_forget = projected[4].astype(jnp.bfloat16)
    rec_input = projected[5].astype(jnp.bfloat16)
    att_out = attention(att_query, key_value, score_offset)
    rec_out = recurrence(rec_query, rec_forget, rec_input, lower_bound, decay_shift, rec_gain)
    outputs = (
        lax.all_gather(att_out_weight, "sp", axis=1, tiled=True),
        lax.all_gather(rec_out_weight, "sp", axis=1, tiled=True),
    )
    att_rows, rec_rows = outputs
    return lax.psum_scatter(
        (
            jnp.dot(att_out, att_rows, preferred_element_type=jnp.float32)
            + jnp.dot(rec_out, rec_rows, preferred_element_type=jnp.float32)
        ).astype(jnp.bfloat16),
        "tp",
        scatter_dimension=0,
        tiled=True,
    )


MESH = pl.DeviceIdType.MESH
STEP = 32


def dot_nt(a, b):
    return lax.dot_general(a, b, (((1,), (1,)), ((), ())), preferred_element_type=jnp.float32)


def dot_tn(a, b):
    return lax.dot_general(a, b, (((0,), (0,)), ((), ())), preferred_element_type=jnp.float32)


def dot_nn(a, b):
    return jnp.dot(a, b, preferred_element_type=jnp.float32)


def remote(src, dst, send_sem, recv_sem, target):
    return pltpu.make_async_remote_copy(
        src_ref=src,
        dst_ref=dst,
        send_sem=send_sem,
        recv_sem=recv_sem,
        device_id=target,
        device_id_type=MESH,
    )


SUB = 32
ROWS8 = 8
LAST = 64
PROFILE = False


def scope(name):
    return jax.named_scope(name) if PROFILE else contextlib.nullcontext()


def stick_block(first, rows, j, group, x, offset_ref):
    block = 128
    q, base = first // block, first % block
    low = lax.broadcasted_iota(jnp.int32, (block, block), 0)
    high = lax.broadcasted_iota(jnp.int32, (block, block), 1)
    later = (low > high).astype(jnp.bfloat16)
    row = lax.broadcasted_iota(jnp.int32, (rows, block), 0) + base
    col = lax.broadcasted_iota(jnp.int32, (rows, block), 1)
    visible = jnp.concatenate([col < row] * group, axis=0)
    offset = jnp.concatenate(
        [jnp.full((rows, block), offset_ref[j * group + g], jnp.float32) for g in range(group)],
        axis=0,
    )
    queries = x[first:first + rows, :group * HEAD]
    queries = jnp.concatenate([queries[:, g * HEAD:(g + 1) * HEAD] for g in range(group)], axis=0)
    run = jnp.zeros((group * rows, 1), jnp.float32)
    summed = jnp.zeros((group * rows, HEAD), jnp.float32)
    for c in range(q, -1, -1):
        keys = x[c * block:(c + 1) * block, group * HEAD:(group + 1) * HEAD]
        values = x[c * block:(c + 1) * block, (group + 1) * HEAD:(group + 2) * HEAD]
        score = dot_nt(queries, keys) * HEAD ** (-0.5) + offset
        keep = -(jnp.maximum(score, 0.0) + jnp.log(1.0 + jnp.exp(-jnp.abs(score))))
        gate = score + keep
        if c == q:
            keep = jnp.where(visible, keep, 0.0)
        top = keep.astype(jnp.bfloat16)
        rest = (keep - top.astype(jnp.float32)).astype(jnp.bfloat16)
        tail = dot_nn(top, later) + dot_nn(rest, later)
        weight = jnp.exp(gate + tail + run)
        if c == q:
            weight = jnp.where(visible, weight, 0.0)
        summed = summed + dot_nn(weight.astype(jnp.bfloat16), values)
        run = run + jnp.sum(keep, axis=1, keepdims=True)
    return jnp.concatenate(
        [summed[g * rows:(g + 1) * rows] for g in range(group)], axis=1
    ).astype(jnp.bfloat16)


def state_block(begin, rows, x, first, bound, gain, shift_ref, state_ref):
    gap = 1.0 - bound
    low = lax.broadcasted_iota(jnp.int32, (rows, rows), 0)
    high = lax.broadcasted_iota(jnp.int32, (rows, rows), 1)
    upto = ((high <= low) & (high // STEP == low // STEP)).astype(jnp.float32)
    lower = (
        lax.broadcasted_iota(jnp.int32, (STEP, STEP), 0)
        >= lax.broadcasted_iota(jnp.int32, (STEP, STEP), 1)
    )
    state = jnp.zeros((REC_VAL, REC_KEY), jnp.float32) if begin == 0 else state_ref[...]
    at = slice(begin, begin + rows)
    query = x[at, first:first + REC_KEY].astype(jnp.float32)
    logit = x[at, first + REC_KEY:first + 2 * REC_KEY].astype(jnp.float32)
    value = x[at, first + 2 * REC_KEY:first + 2 * REC_KEY + REC_VAL]
    log_decay = jnp.log(bound + gap * jax.nn.sigmoid(logit)) + shift_ref[at].astype(jnp.float32)
    keyed = gap * jax.nn.sigmoid(-logit)
    query = query * jax.nn.sigmoid(query)
    running = jnp.dot(upto, log_decay, precision=TOP_PRECISION, preferred_element_type=jnp.float32)
    outs = []
    for i in range(rows // STEP):
        it = slice(i * STEP, (i + 1) * STEP)
        cumulative, q, k, v = running[it], query[it], keyed[it], value[it]
        middle = cumulative[STEP // 2 - 1:STEP // 2]
        last = cumulative[STEP - 1:STEP]
        score = dot_nt(
            (q * jnp.exp(cumulative - middle)).astype(jnp.bfloat16),
            (k * jnp.exp(middle - cumulative)).astype(jnp.bfloat16),
        )
        score = jnp.where(lower, score, 0.0).astype(jnp.bfloat16)
        raw = dot_nn(score, v) + dot_nt(
            (q * jnp.exp(cumulative)).astype(jnp.bfloat16), state.astype(jnp.bfloat16)
        )
        state = state * jnp.exp(last) + dot_tn(
            v, (k * jnp.exp(last - cumulative)).astype(jnp.bfloat16)
        )
        scale = lax.rsqrt(jnp.mean(raw * raw, axis=1, keepdims=True) + EPS)
        outs.append((raw * scale * gain).astype(jnp.bfloat16))
    state_ref[...] = state
    return jnp.concatenate(outs, axis=0)


def units_of(n, rows):
    seq = n * rows
    whole = [(k * rows, rows) for k in range(n - 2)]
    return whole + [(r, LAST) for r in range((n - 2) * rows, seq, LAST)]


def layer_kernel(
    n, nt, group,
    tok_ref, gain_ref, aq_ref, ak_ref, av_ref, rq_ref, rf_ref, ri_ref, shift_ref,
    wa_ref, wr_ref, offset_ref, bound_ref, rec_gain_ref,
    out_ref,
    tokens, gains, bounds, rec_gains, weights, outs, wide_shift, own_shift, tbuf, shifts, squares, scales,
    part, sent, came, x, state, heads, shares, landed, mixed,
    l_sem, a_send, a_recv, b_send, b_recv, d_send, d_recv, q_send, q_recv,
    c_send, c_recv, e_send, e_recv, f_send, f_recv, g_send, g_recv,
):
    s, t = lax.axis_index("sp"), lax.axis_index("tp")
    rows, feats = own_shift.shape[0], tokens.shape[-1]
    piece = rows // nt
    width = x.shape[1]
    att_width = (group + 2) * HEAD
    wide = group * HEAD
    cols = outs.shape[-1]
    subs = rows // SUB
    ends = (0, n - 1)
    f32, bf16 = jnp.float32, jnp.bfloat16
    units = units_of(n, rows)
    nu = len(units)

    load_tokens = pltpu.make_async_copy(tok_ref, tokens, l_sem.at[0])
    load_gain = pltpu.make_async_copy(
        gain_ref.at[:, pl.ds(pl.multiple_of(s * feats, feats), feats)], gains, l_sem.at[1]
    )
    load_weights = []
    first = 0
    for ref, size in (
        (aq_ref, wide), (ak_ref, HEAD), (av_ref, HEAD),
        (rq_ref, REC_KEY), (rf_ref, REC_KEY), (ri_ref, REC_VAL),
    ):
        for i in range(2):
            load_weights.append(
                pltpu.make_async_copy(
                    ref.at[pl.ds(i * size, size)], weights.at[i, pl.ds(first, size)], l_sem.at[2]
                )
            )
        first += size
    load_shift = pltpu.make_async_copy(shift_ref, wide_shift, l_sem.at[3])
    load_bounds = pltpu.make_async_copy(bound_ref, bounds, l_sem.at[4])
    load_rec_gains = pltpu.make_async_copy(rec_gain_ref, rec_gains, l_sem.at[5])
    load_outs = [
        pltpu.make_async_copy(ref, outs.at[o], l_sem.at[6]) for o, ref in enumerate((wa_ref, wr_ref))
    ]

    load_tokens.start()
    barrier = pltpu.get_barrier_semaphore()
    for a in range(n):
        for b in range(nt):
            if a or b:
                pl.semaphore_signal(
                    barrier, inc=1,
                    device_id={"sp": lax.rem(s + a, n), "tp": lax.rem(t + b, nt)},
                    device_id_type=MESH,
                )
    for load in (
        load_shift, load_gain, *load_weights, load_bounds, load_rec_gains, *load_outs
    ):
        load.start()
    load_tokens.wait()
    with scope("barrier"):
        pl.semaphore_wait(barrier, n * nt - 1)

    def plane(v):
        others = [i for i in range(2) if v != ends[i]]
        mine = [i for i in range(2) if v == ends[i]]
        order = (1, 0) if v < n // 2 else (0, 1)

        def parts_of(k):
            return range(subs) if k == 0 else (slice(None),)

        def slot(c):
            return 0 if isinstance(c, slice) else c

        def lane_of(k, c):
            return c if k == 0 else subs + k - 1

        def first_copy(c, j):
            return remote(
                tokens.at[c, j], tbuf.at[v, c, j], a_send, a_recv.at[lane_of(v, c)],
                {"sp": t, "tp": j},
            )

        def first_here(c):
            return pltpu.make_async_copy(
                tokens.at[c, v], tbuf.at[v, c, v], a_recv.at[lane_of(v, c)]
            )

        def send_first(when):
            pl.when(when)(send_first_now)

        def send_first_now():
            for c in parts_of(v):
                for j in range(nt):
                    if j == v:
                        pl.when(t != v)(lambda: first_copy(c, j).start())
                        pl.when(t == v)(lambda: first_here(c).start())
                    else:
                        first_copy(c, j).start()

        def second_copy(k, c, d):
            return remote(
                tbuf.at[k, c, t], tbuf.at[k, c, t],
                b_send, b_recv.at[lane_of(k, c)],
                {"tp": lax.rem(t + d, nt)},
            )

        def relay(k, c):
            with scope(f"relay{k}"):
                remote(
                    tokens.at[c, 0], tbuf.at[k, c, t], a_send, a_recv.at[lane_of(k, c)],
                    {"sp": (v + 1) % n},
                ).wait_recv()
            for d in range(1, nt):
                second_copy(k, c, d).start()

        def square_copy(k, i):
            return remote(
                squares.at[v, k], squares.at[v, k], q_send.at[i], q_recv.at[k],
                {"sp": ends[i]},
            )

        def chain_copy(i, c):
            to = v - 1 if i == 0 else v + 1
            return remote(
                sent.at[i, pl.ds(c * SUB, SUB)], came.at[i, pl.ds(c * SUB, SUB)],
                c_send.at[i], c_recv.at[i, c], {"sp": to},
            )

        def project(k, c):
            with scope(f"wtok{k}"):
                most = tbuf.at[k, c, pl.ds(0, nt - 1)]
                remote(
                    most, most, b_send, b_recv.at[lane_of(k, c)], {"tp": lax.rem(t + 1, nt)}
                ).wait_recv()
            size = rows if isinstance(c, slice) else SUB
            begin = k * rows + slot(c) * SUB
            raw = tbuf[k, c].reshape(size, feats).astype(f32)
            scaled = (raw * gains[...]).astype(bf16)
            for i in order:
                product = dot_nt(scaled, weights[i])
                if v == ends[1 - i]:
                    for r in range(size // SUB):
                        at = begin + r * SUB
                        sent[i, pl.ds(at, SUB)] = product[r * SUB:(r + 1) * SUB].astype(bf16)
                        chain_copy(i, at // SUB).start()
                else:
                    part[i, pl.ds(begin, size)] = product

        def square(k):
            raw = tbuf[k].reshape(rows, feats).astype(f32)
            total = jnp.sum(raw * raw, axis=1, keepdims=True)
            flat = jnp.transpose(jnp.broadcast_to(total, (rows, 128)))
            squares[v, k] = flat[:8]
            for i in others:
                square_copy(k, i).start()

        def shift_copy(i):
            return remote(
                own_shift.at[:, pl.ds(i * REC_KEY, REC_KEY)], shifts.at[pl.ds(v * rows, rows)],
                d_send.at[i], d_recv.at[v], {"sp": ends[i]},
            )

        def shift_here(i):
            return pltpu.make_async_copy(
                own_shift.at[:, pl.ds(i * REC_KEY, REC_KEY)], shifts.at[pl.ds(v * rows, rows)],
                d_recv.at[v],
            )

        def send_shift(i):
            if v == ends[i]:
                shift_here(i).start()
            else:
                shift_copy(i).start()

        def forward(i, c):
            with scope(f"chain{i}_{c}"):
                chain_copy(i, c).wait_recv()
            at = (i, pl.ds(c * SUB, SUB))
            sent[at] = (part[at] + came[at].astype(f32)).astype(bf16)
            chain_copy(i, c).start()

        def head_copy(i, u, to):
            at = (i, pl.ds(units[u][0], units[u][1]))
            return remote(
                heads.at[at], heads.at[at], e_send.at[to], e_recv.at[i, u], {"sp": to}
            )

        def near(i):
            return 1 if i == 0 else n - 2

        def between(i):
            return [p for p in range(1, n - 1) if p != near(i)]

        def direct(i, u):
            return MODES[i][units[u][0] // rows] == 2

        def relayed(i, u):
            return MODES[i][units[u][0] // rows] == 0

        def head_targets(i, u):
            far = ends[1 - i]
            if relayed(i, u):
                return [] if v == far else [v + 1 if i == 0 else v - 1]
            if v == ends[i]:
                if direct(i, u):
                    return [far, *between(i), near(i)]
                return [near(i), far]
            if v == near(i) and not direct(i, u):
                return between(i)
            return []

        def send_heads(i, u, to):
            head_copy(i, u, to).start()

        def wait_heads(i, u):
            with scope(f"whead{i}_{u}"):
                head_copy(i, u, ends[i]).wait_recv()

        def mix(u):
            e = mine[0]
            begin, size = units[u]
            k = begin // rows
            span = pl.ds(begin, size)
            with scope(f"wmix{u}"):
                for c in range(begin // SUB, (begin + size) // SUB):
                    chain_copy(e, c).wait_recv()
            if begin % rows == 0:
                most = squares.at[pl.ds(0, n - 1), k]
                remote(most, most, q_send.at[e], q_recv.at[k], {"sp": ends[1 - e]}).wait_recv()
                remote(
                    own_shift.at[:, pl.ds(e * REC_KEY, REC_KEY)],
                    shifts.at[pl.ds(k * rows, rows)], d_send.at[e], d_recv.at[k],
                    {"sp": ends[1 - e]},
                ).wait_recv()
                total = squares[0, k, :1]
                for p in range(1, n):
                    total = total + squares[p, k, :1]
                inv_rms = lax.rsqrt(total / (feats * n) + EPS)
                scales[...] = jnp.transpose(jnp.broadcast_to(inv_rms, (128, rows)))
            inv_rms = scales[pl.ds(begin % rows, size)]
            for c in range(width // 128):
                lane = pl.ds(c * 128, 128)
                result = part[e, span, lane] + came[e, span, lane].astype(f32)
                x[span, lane] = (result * inv_rms).astype(bf16)
            with scope(f"stick{u}"):
                heads[e, span, pl.ds(0, wide)] = stick_block(
                    begin, size, e, group, x, offset_ref
                )
            with scope(f"state{u}"):
                heads[e, span, pl.ds(wide, REC_VAL)] = state_block(
                    begin, size, x, att_width,
                    bounds[:, pl.ds(e * REC_KEY, REC_KEY)],
                    rec_gains[:, pl.ds(e * REC_VAL, REC_VAL)], shifts, state,
                )

        def share_copy(k, b):
            to = lax.rem(t + b, nt)
            return remote(
                shares.at[k, to], landed.at[k, b], f_send, f_recv.at[k], {"tp": to}
            )

        def multiply(u):
            begin, size = units[u]
            k = begin // rows
            span = pl.ds(begin, size)
            total = None
            for i in range(2):
                for o, at, deep in ((0, 0, wide), (1, wide, REC_VAL)):
                    term = dot_nn(heads[i, span, pl.ds(at, deep)], outs[o, pl.ds(i * deep, deep)])
                    total = term if total is None else total + term
            total = total.astype(bf16)
            if size == rows:
                shares[k] = total.reshape(nt, piece, cols)
                for b in range(1, nt):
                    share_copy(k, b).start()
            else:
                for j in range(begin % rows // piece, (begin % rows + size) // piece):
                    at = j * piece - begin % rows
                    shares[k, j] = total[at:at + piece]
                    b = lax.rem(j - t + nt, nt)
                    pl.when(t != j)(lambda: share_copy(k, b).start())

        place = out_ref.at[:, pl.ds(v * cols, cols)]

        def final_copy(k):
            return remote(mixed.at[k], place, g_send, g_recv, {"sp": k})

        def final_here():
            return pltpu.make_async_copy(mixed.at[v], place, g_recv)

        def combine(k):
            with scope(f"wshare{k}"):
                most = pl.ds(1, nt - 1)
                remote(
                    shares.at[k, most], landed.at[k, most], f_send, f_recv.at[k],
                    {"tp": lax.rem(t + 1, nt)},
                ).wait_recv()
            result = shares[k, t].astype(f32)
            for b in range(1, nt):
                result = result + landed[k, b].astype(f32)
            mixed[k] = result.astype(bf16)
            if k == v:
                final_here().start()
            else:
                final_copy(k).start()

        def projection_loaded():
            load_gain.wait()
            pltpu.make_async_copy(weights, weights, l_sem.at[2]).wait()

        def rest_loaded():
            load_bounds.wait()
            load_rec_gains.wait()
            pltpu.make_async_copy(outs, outs, l_sem.at[6]).wait()

        events = []

        def event(time, *call):
            events.append((time, len(events), call))

        starts = (START0, START1)
        hops = (n - 1 - v, v)
        whole = slice(None)
        event(5.9, projection_loaded)
        def round_shift():
            own_shift[...] = wide_shift[...].astype(bf16)

        event(0.1, load_shift.wait)
        event(0.15, round_shift)
        event(15.0, rest_loaded)
        soon = t < v
        if v < n // 2:
            soon = soon | (t == n - 1)
        if v == 0:
            soon = t >= 0
        event(0.0, send_first, soon)
        for c in range(subs):
            event(4.0 + 0.1 * c, relay, 0, c)
        event(4.05, send_first, jnp.logical_not(soon))
        for c in range(subs):
            event(6.0 + 0.1 * c, project, 0, c)
        event(0.2, send_shift, 0)
        event(4.4 if 0 < v < n - 1 else 0.2, send_shift, 1)
        event(7.1, square, 0)
        ready = [6.5]
        for k in range(1, n):
            event(6.05 if k == 1 else 9.0 + 0.1 * k, relay, k, whole)
            at = (TOKENS if v in ends else TOKENS_MID)[k - 1]
            event(at, project, k, whole)
            event(at + 0.1, square, k)
            ready.append(at + 0.01)
        chain_end = 0.0
        if v not in ends:
            for i in range(2):
                for c in range(n * subs):
                    at = max(starts[i] + hops[i] * HOP + CHUNK * c, ready[c // subs])
                    event(at, forward, i, c)
                    chain_end = max(chain_end, at)
        def distance(i, p):
            return p if i == 0 else n - 1 - p

        def leaves(i, u, to):
            last = starts[1 - i] + distance(i, to) * HOP + CHUNK * (n * subs - 1)
            return max(done[i][u] - 0.1, last - FAR)

        done = [[0.0] * nu, [0.0] * nu]
        for i in range(2):
            at = 0.0
            for u, (begin, size) in enumerate(units):
                last = (begin + size) // SUB - 1
                arrive = max(at, starts[i] + (n - 1) * HOP + CHUNK * last)
                at = arrive + (1.8 if size == rows else 1.45)
                done[i][u] = at
                if v == ends[i]:
                    event(arrive, mix, u)
                    for to in head_targets(i, u):
                        event(leaves(i, u, to), send_heads, i, u, to)
        for u, (begin, size) in enumerate(units):
            k = begin // rows
            latest = max(done[0][u], done[1][u], chain_end + 0.01)
            for i in others:
                load = 1.4 * size / rows
                away = distance(i, v)
                if relayed(i, u):
                    at = leaves(i, u, near(i)) + (3.0 + load) * away
                elif direct(i, u):
                    at = leaves(i, u, v) + 2.8 + 0.45 * away + (n - away) * load
                elif v in between(i):
                    at = leaves(i, u, near(i)) + 6.5 + 2 * load
                else:
                    at = leaves(i, u, v) + 2.8 + 0.45 * away + load
                if v in ends:
                    at = max(at, done[mine[0]][nu - 1] + 0.01)
                elif v == 1 and i == 0 and relayed(i, u):
                    at -= 0.2
                else:
                    at = max(at, chain_end + 0.01)
                event(at, wait_heads, i, u)
                for to in head_targets(i, u):
                    event(at, send_heads, i, u, to)
                latest = max(latest, at)
            event(latest + 0.02, multiply, u)
            if begin + size == (k + 1) * rows:
                event(latest + 4.5, combine, k)
        for _, _, (call, *args) in sorted(events, key=lambda e: e[:2]):
            call(*args)

        with scope("wfinal"):
            pltpu.make_async_copy(out_ref, out_ref, g_recv).wait()

        with scope("wsend"):
            def sent_all(src, sem):
                remote(src, src, sem, a_recv.at[0], {"sp": (v + 1) % n}).wait_send()

            pl.when(t != v)(lambda: sent_all(tokens, a_send))
            pl.when(t == v)(lambda: sent_all(tokens.at[:, pl.ds(0, nt - 1)], a_send))
            sent_all(tbuf.at[:, :, pl.ds(0, nt - 1)], b_send)
            sent_all(shares.at[:, pl.ds(0, nt - 1)], f_send)
            sent_all(mixed.at[pl.ds(0, n - 1)], g_send)
            for i in others:
                sent_all(own_shift.at[:, pl.ds(i * REC_KEY, REC_KEY)], d_send.at[i])
                sent_all(squares.at[v], q_send.at[i])
                sent_all(sent.at[i], c_send.at[i])
            for to in range(n):
                spans = [
                    units[u] for i in range(2) for u in range(nu) if to in head_targets(i, u)
                ]
                if spans:
                    begin = spans[0][0]
                    size = sum(size for _, size in spans)
                    sent_all(heads.at[0, pl.ds(begin, size)], e_send.at[to])

    for v in range(n):
        if v in ends:
            @pl.when(s == v)
            def _():
                x[...] = jnp.zeros_like(x)
                plane(v)
        else:
            pl.when(s == v)(functools.partial(plane, v))


START0, START1, HOP, CHUNK = 8.0, 6.3, 3.6, 0.88
FAR = 3.2
MODES = ((0, 1, 1, 1), (0, 0, 1, 1))
TOKENS = (10.5, 11.5, 12.5)
TOKENS_MID = (10.5, 14.0, 16.5)


def stationary_fits(args):
    n, nt = lax.axis_size("sp"), lax.axis_size("tp")
    tokens, att_q, att_k, rec_i = args[0], args[2], args[3], args[7]
    rows, feats = tokens.shape
    return (
        n == nt
        and n >= 3
        and att_k.shape[0] // HEAD == 2
        and rec_i.shape[0] // REC_VAL == 2
        and (att_q.shape[0] // att_k.shape[0]) * HEAD == 128
        and feats == att_q.shape[1]
        and rows == 128
        and rows == SUB * nt
        and SUB == ROWS8 * nt
    )


def stationary(*args):
    n, nt = lax.axis_size("sp"), lax.axis_size("tp")
    tokens, norm_gain, att_q, att_k = args[:4]
    score_offset, lower_bound, decay_shift, rec_gain = args[10:]
    rows, feats = tokens.shape
    seq = rows * n
    deep, cols = args[8].shape
    group = att_q.shape[0] // att_k.shape[0]
    width = (group + 2) * HEAD + 2 * REC_KEY + REC_VAL
    wide = group * HEAD + REC_VAL
    piece = rows // nt
    chunks = seq // SUB
    subs = rows // SUB
    nu = len(units_of(n, rows))
    bf16, f32 = jnp.bfloat16, jnp.float32
    dma = pltpu.SemaphoreType.DMA
    vmem = pl.BlockSpec(memory_space=pltpu.VMEM)
    hbm = pl.BlockSpec(memory_space=pl.ANY)
    smem = pl.BlockSpec(memory_space=pltpu.SMEM)
    return pl.pallas_call(
        functools.partial(layer_kernel, n, nt, group),
        out_shape=pltpu.VMEM((piece, cols * n), bf16),
        in_specs=[hbm] * 11 + [smem, hbm, hbm],
        out_specs=vmem,
        scratch_shapes=[
            pltpu.VMEM((subs, nt, ROWS8, feats), bf16),
            pltpu.VMEM((1, feats), f32),
            pltpu.VMEM((1, 2 * REC_KEY), f32),
            pltpu.VMEM((1, 2 * REC_VAL), f32),
            pltpu.VMEM((2, width, feats), bf16),
            pltpu.VMEM((2, deep, cols), bf16),
            pltpu.VMEM((rows, 2 * REC_KEY), f32),
            pltpu.VMEM((rows, 2 * REC_KEY), bf16),
            pltpu.VMEM((n, subs, nt, ROWS8, feats), bf16),
            pltpu.VMEM((seq, REC_KEY), bf16),
            pltpu.VMEM((n, n, 8, rows), f32),
            pltpu.VMEM((rows, 128), f32),
            pltpu.VMEM((2, seq, width), f32),
            pltpu.VMEM((2, seq, width), bf16),
            pltpu.VMEM((2, seq, width), bf16),
            pltpu.VMEM((seq, width), bf16),
            pltpu.VMEM((REC_VAL, REC_KEY), f32),
            pltpu.VMEM((2, seq, wide), bf16),
            pltpu.VMEM((n, nt, piece, cols), bf16),
            pltpu.VMEM((n, nt, piece, cols), bf16),
            pltpu.VMEM((n, piece, cols), bf16),
            dma((7,)), dma, dma((subs + n - 1,)), dma, dma((subs + n - 1,)), dma((2,)), dma((n,)),
            dma((2,)), dma((n,)), dma((2,)), dma((2, chunks)), dma((n,)), dma((2, nu)),
            dma, dma((n,)), dma, dma,
        ],
        compiler_params=pltpu.CompilerParams(collective_id=0, has_side_effects=True),
        name="layer",
    )(
        tokens.reshape(subs, nt, ROWS8, feats), norm_gain.reshape(1, -1), *args[2:8], decay_shift,
        args[8], args[9],
        score_offset, lower_bound.reshape(1, -1), rec_gain.reshape(1, -1),
    )


def on_device(*args):
    if stationary_fits(args):
        return stationary(*args)
    return gathered_plan(*args)


def solution(mesh):
    in_specs = (
        P(("grp", "sp"), "tp"),
        P(),
        P("tp", "sp"),
        P("tp", "sp"),
        P("tp", "sp"),
        P("tp", "sp"),
        P("tp", "sp"),
        P("tp", "sp"),
        P("tp", "sp"),
        P("tp", "sp"),
        P("tp"),
        P("tp"),
        P(("grp", "sp"), "tp"),
        P("tp"),
    )
    out_specs = P(("grp", "sp", "tp"), None)
    return jax.shard_map(
        on_device, mesh=mesh, in_specs=in_specs, out_specs=out_specs, check_vma=False
    )
```

```python
import contextlib
import functools

import jax
import jax.numpy as jnp
from jax import lax
from jax.experimental import pallas as pl
from jax.experimental.pallas import tpu as pltpu
from jax.sharding import PartitionSpec as P

HEAD = 64
REC_KEY = 128
REC_VAL = 128
SPAN = 64


EPS = 1e-06
TOP_PRECISION = lax.Precision.HIGHEST


def entering(x, axis, combine, identity):
    count, here = (lax.axis_size(axis), lax.axis_index(axis))
    everything = jax.tree.map(
        lambda part, kind: lax.all_gather(part.astype(kind), axis), x, (jnp.bfloat16, jnp.bfloat16)
    )
    start = jax.tree.map(
        lambda part, zero: jnp.broadcast_to(jnp.asarray(zero, part.dtype), part.shape), x, identity
    )

    def entering_turn(k, before):
        reached = k < here
        new = combine(
            before, jax.tree.map(lambda part, own: part[k].astype(own.dtype), everything, x)
        )
        return jax.tree.map(lambda a, b: jnp.where(reached, a, b), new, before)

    return lax.fori_loop(0, count, entering_turn, start)


def make_fold(norm_gain, weights, carry, piece):
    elementwise_sq, totals = carry
    raw = piece.astype(jnp.float32)
    scaled = (raw * norm_gain[None, :]).astype(jnp.bfloat16)
    elementwise_sq = jnp.sum(raw * raw, axis=1)
    updated = []
    for total, weight in zip(totals, weights):
        updated.append(
            lax.dot_general(
                scaled, weight, (((1,), (1,)), ((), ())), preferred_element_type=jnp.float32
            )
        )
    return (elementwise_sq, tuple(updated))


def project_all(tokens, norm_gain, weights):
    rows = tokens.shape[0]
    width = weights[0].shape[1]
    start_carry = (
        jnp.zeros((rows,), jnp.float32),
        tuple((jnp.zeros((rows, weight.shape[0]), jnp.float32) for weight in weights)),
    )
    elementwise_sq, totals = make_fold(
        norm_gain, weights, start_carry, lax.all_gather(tokens, "tp", axis=1, tiled=True)
    )
    inv_rms = lax.rsqrt(elementwise_sq / width + EPS)
    return tuple((total * inv_rms[:, None] for total in totals))


def attention(att_query, key_value, score_offset):
    rows = att_query.shape[0]
    gathered = lax.all_gather(key_value, "sp", axis=0, tiled=True)
    seq = gathered.shape[0]
    kv_heads = key_value.shape[1] // (2 * HEAD)
    q_heads = att_query.shape[1] // HEAD
    group = q_heads // kv_heads
    kv_width = kv_heads * HEAD
    queries = att_query.reshape(rows, kv_heads, group, HEAD)
    offsets = score_offset.reshape(kv_heads, group)
    kblock = min(1024, seq)
    first_row = lax.axis_index("sp") * rows
    query_pos = first_row + jnp.arange(rows, dtype=jnp.int32)
    count = (first_row + rows - 1) // kblock + 1

    def attention_turn(step, carry):
        summed, run = carry
        block_start = (count - 1 - step) * kblock
        block = lax.dynamic_slice_in_dim(gathered, block_start, kblock, 0)
        keys = block[:, :kv_width].reshape(kblock, kv_heads, HEAD)
        values = block[:, kv_width:].reshape(kblock, kv_heads, HEAD)
        score = (
            jnp.einsum("tkgd,skd->tkgs", queries, keys, preferred_element_type=jnp.float32)
            * HEAD ** (-0.5)
            + offsets[None, :, :, None]
        )
        key_pos = block_start + jnp.arange(kblock, dtype=jnp.int32)
        visible = (key_pos[None, :] < query_pos[:, None])[:, None, None, :]
        keep = jnp.where(visible, jax.nn.log_sigmoid(-score), 0.0)
        tail = lax.cumsum(keep, axis=3, reverse=True) - keep
        weight = jnp.where(
            visible, jnp.exp(jax.nn.log_sigmoid(score) + tail + run[..., None]), 0.0
        ).astype(jnp.bfloat16)
        summed = summed + jnp.einsum(
            "tkgs,skd->tkgd", weight, values, preferred_element_type=jnp.float32
        )
        return (summed, run + jnp.sum(keep, axis=3))

    start_carry = (
        jnp.zeros((rows, kv_heads, group, HEAD), jnp.float32),
        jnp.zeros((rows, kv_heads, group), jnp.float32),
    )
    summed, _ = lax.fori_loop(0, count, attention_turn, start_carry)
    return summed.reshape(rows, q_heads * HEAD).astype(jnp.bfloat16)


def block_pass(carry, inputs):
    state_matrix, prefix = carry
    query_rows, log_decay, keyed_values, value_rows = inputs
    span = query_rows.shape[0]
    cumulative_log = jnp.cumsum(log_decay, axis=0)
    lower = jnp.arange(span, dtype=jnp.int32)[:, None] >= jnp.arange(span, dtype=jnp.int32)[None, :]
    diff = cumulative_log[:, None] - cumulative_log[None, :]
    decay = jnp.exp(jnp.where(lower[:, :, None, None], diff, -jnp.inf))
    score = jnp.einsum(
        "thk,tshk,shk->ths", query_rows, decay, keyed_values, precision=TOP_PRECISION
    )
    inner = jnp.einsum("ths,shv->thv", score, value_rows, precision=TOP_PRECISION)
    outer_product = jnp.einsum(
        "ril,ilc->ric", query_rows * jnp.exp(cumulative_log), state_matrix, precision=TOP_PRECISION
    )
    final_state = cumulative_log[-1]
    state_matrix = state_matrix * jnp.exp(final_state)[:, :, None] + jnp.einsum(
        "iag,iax->agx",
        keyed_values * jnp.exp(final_state[None] - cumulative_log),
        value_rows,
        precision=TOP_PRECISION,
    )
    reach_limit = query_rows * jnp.exp(cumulative_log + prefix[None])
    return ((state_matrix, prefix + final_state), (inner + outer_product, reach_limit))


def chain(earlier, later):
    return (earlier[0] * later[0], earlier[1] * later[0][:, :, None] + later[1])


def recurrence(rec_query, rec_forget, rec_input, lower_bound, decay_shift, rec_gain):
    rows = rec_query.shape[0]
    heads = rec_gain.shape[0] // REC_VAL
    logit = rec_forget.astype(jnp.float32)
    gap = 1.0 - lower_bound
    log_decay = jnp.log(lower_bound + gap * jax.nn.sigmoid(logit)) + decay_shift
    keyed_values = gap * jax.nn.sigmoid(-logit)
    query_rows = jax.nn.silu(rec_query.astype(jnp.float32))
    blocks = rows // SPAN

    def split(array, depth):
        return array.reshape(blocks, SPAN, heads, depth)

    start_carry = (
        jnp.zeros((heads, REC_KEY, REC_VAL), jnp.float32),
        jnp.zeros((heads, REC_KEY), jnp.float32),
    )
    (state_matrix, total), (local, reach_limit) = lax.scan(
        block_pass,
        start_carry,
        (
            split(query_rows, REC_KEY),
            split(log_decay, REC_KEY),
            split(keyed_values, REC_KEY),
            split(rec_input.astype(jnp.float32), REC_VAL),
        ),
    )
    identity = (
        jnp.ones((heads, REC_KEY), jnp.float32),
        jnp.zeros((heads, REC_KEY, REC_VAL), jnp.float32),
    )
    incoming_state = entering((jnp.exp(total), state_matrix), "sp", chain, identity)
    running_memory = jnp.einsum(
        "lida,dao->lido", reach_limit, incoming_state[1], precision=TOP_PRECISION
    )
    rec_raw = (local + running_memory).reshape(rows, heads, REC_VAL)
    rescaled_input = (
        rec_raw
        * lax.rsqrt(jnp.mean(rec_raw * rec_raw, axis=2, keepdims=True) + EPS)
        * rec_gain.reshape(heads, REC_VAL)
    )
    return rescaled_input.reshape(rows, heads * REC_VAL).astype(jnp.bfloat16)


def gathered_plan(
    tokens,
    norm_gain,
    att_q_weight,
    att_k_weight,
    att_v_weight,
    rec_q_weight,
    rec_f_weight,
    rec_i_weight,
    att_out_weight,
    rec_out_weight,
    score_offset,
    lower_bound,
    decay_shift,
    rec_gain,
):
    inputs = (
        lax.all_gather(att_q_weight, "sp", axis=1, tiled=True),
        lax.all_gather(att_k_weight, "sp", axis=1, tiled=True),
        lax.all_gather(att_v_weight, "sp", axis=1, tiled=True),
        lax.all_gather(rec_q_weight, "sp", axis=1, tiled=True),
        lax.all_gather(rec_f_weight, "sp", axis=1, tiled=True),
        lax.all_gather(rec_i_weight, "sp", axis=1, tiled=True),
    )
    projected = project_all(tokens, norm_gain, inputs)
    att_query = projected[0].astype(jnp.bfloat16)
    key_value = jnp.concatenate(projected[1:3], axis=1).astype(jnp.bfloat16)
    rec_query = projected[3].astype(jnp.bfloat16)
    rec_forget = projected[4].astype(jnp.bfloat16)
    rec_input = projected[5].astype(jnp.bfloat16)
    att_out = attention(att_query, key_value, score_offset)
    rec_out = recurrence(rec_query, rec_forget, rec_input, lower_bound, decay_shift, rec_gain)
    outputs = (
        lax.all_gather(att_out_weight, "sp", axis=1, tiled=True),
        lax.all_gather(rec_out_weight, "sp", axis=1, tiled=True),
    )
    att_rows, rec_rows = outputs
    return lax.psum_scatter(
        (
            jnp.dot(att_out, att_rows, preferred_element_type=jnp.float32)
            + jnp.dot(rec_out, rec_rows, preferred_element_type=jnp.float32)
        ).astype(jnp.bfloat16),
        "tp",
        scatter_dimension=0,
        tiled=True,
    )


MESH = pl.DeviceIdType.MESH
STEP = 32


def dot_nt(a, b):
    return lax.dot_general(a, b, (((1,), (1,)), ((), ())), preferred_element_type=jnp.float32)


def dot_tn(a, b):
    return lax.dot_general(a, b, (((0,), (0,)), ((), ())), preferred_element_type=jnp.float32)


def dot_nn(a, b):
    return jnp.dot(a, b, preferred_element_type=jnp.float32)


def remote(src, dst, send_sem, recv_sem, target):
    return pltpu.make_async_remote_copy(
        src_ref=src,
        dst_ref=dst,
        send_sem=send_sem,
        recv_sem=recv_sem,
        device_id=target,
        device_id_type=MESH,
    )


SUB = 32
ROWS8 = 8
LAST = 64
PROFILE = False


def scope(name):
    return jax.named_scope(name) if PROFILE else contextlib.nullcontext()


def stick_block(first, rows, j, group, x, offset_ref):
    block = 128
    q, base = first // block, first % block
    low = lax.broadcasted_iota(jnp.int32, (block, block), 0)
    high = lax.broadcasted_iota(jnp.int32, (block, block), 1)
    later = (low > high).astype(jnp.bfloat16)
    row = lax.broadcasted_iota(jnp.int32, (rows, block), 0) + base
    col = lax.broadcasted_iota(jnp.int32, (rows, block), 1)
    visible = jnp.concatenate([col < row] * group, axis=0)
    offset = jnp.concatenate(
        [jnp.full((rows, block), offset_ref[j * group + g], jnp.float32) for g in range(group)],
        axis=0,
    )
    queries = x[first:first + rows, :group * HEAD]
    queries = jnp.concatenate([queries[:, g * HEAD:(g + 1) * HEAD] for g in range(group)], axis=0)
    run = jnp.zeros((group * rows, 1), jnp.float32)
    summed = jnp.zeros((group * rows, HEAD), jnp.float32)
    for c in range(q, -1, -1):
        keys = x[c * block:(c + 1) * block, group * HEAD:(group + 1) * HEAD]
        values = x[c * block:(c + 1) * block, (group + 1) * HEAD:(group + 2) * HEAD]
        score = dot_nt(queries, keys) * HEAD ** (-0.5) + offset
        keep = -(jnp.maximum(score, 0.0) + jnp.log(1.0 + jnp.exp(-jnp.abs(score))))
        gate = score + keep
        if c == q:
            keep = jnp.where(visible, keep, 0.0)
        top = keep.astype(jnp.bfloat16)
        rest = (keep - top.astype(jnp.float32)).astype(jnp.bfloat16)
        tail = dot_nn(top, later) + dot_nn(rest, later)
        weight = jnp.exp(gate + tail + run)
        if c == q:
            weight = jnp.where(visible, weight, 0.0)
        summed = summed + dot_nn(weight.astype(jnp.bfloat16), values)
        run = run + jnp.sum(keep, axis=1, keepdims=True)
    return jnp.concatenate(
        [summed[g * rows:(g + 1) * rows] for g in range(group)], axis=1
    ).astype(jnp.bfloat16)


def state_block(begin, rows, x, first, bound, gain, shift_ref, state_ref):
    gap = 1.0 - bound
    low = lax.broadcasted_iota(jnp.int32, (rows, rows), 0)
    high = lax.broadcasted_iota(jnp.int32, (rows, rows), 1)
    upto = ((high <= low) & (high // STEP == low // STEP)).astype(jnp.float32)
    lower = (
        lax.broadcasted_iota(jnp.int32, (STEP, STEP), 0)
        >= lax.broadcasted_iota(jnp.int32, (STEP, STEP), 1)
    )
    state = jnp.zeros((REC_VAL, REC_KEY), jnp.float32) if begin == 0 else state_ref[...]
    at = slice(begin, begin + rows)
    query = x[at, first:first + REC_KEY].astype(jnp.float32)
    logit = x[at, first + REC_KEY:first + 2 * REC_KEY].astype(jnp.float32)
    value = x[at, first + 2 * REC_KEY:first + 2 * REC_KEY + REC_VAL]
    log_decay = jnp.log(bound + gap * jax.nn.sigmoid(logit)) + shift_ref[at].astype(jnp.float32)
    keyed = gap * jax.nn.sigmoid(-logit)
    query = query * jax.nn.sigmoid(query)
    running = jnp.dot(upto, log_decay, precision=TOP_PRECISION, preferred_element_type=jnp.float32)
    outs = []
    for i in range(rows // STEP):
        it = slice(i * STEP, (i + 1) * STEP)
        cumulative, q, k, v = running[it], query[it], keyed[it], value[it]
        middle = cumulative[STEP // 2 - 1:STEP // 2]
        last = cumulative[STEP - 1:STEP]
        score = dot_nt(
            (q * jnp.exp(cumulative - middle)).astype(jnp.bfloat16),
            (k * jnp.exp(middle - cumulative)).astype(jnp.bfloat16),
        )
        score = jnp.where(lower, score, 0.0).astype(jnp.bfloat16)
        raw = dot_nn(score, v) + dot_nt(
            (q * jnp.exp(cumulative)).astype(jnp.bfloat16), state.astype(jnp.bfloat16)
        )
        state = state * jnp.exp(last) + dot_tn(
            v, (k * jnp.exp(last - cumulative)).astype(jnp.bfloat16)
        )
        scale = lax.rsqrt(jnp.mean(raw * raw, axis=1, keepdims=True) + EPS)
        outs.append((raw * scale * gain).astype(jnp.bfloat16))
    state_ref[...] = state
    return jnp.concatenate(outs, axis=0)


def units_of(n, rows):
    seq = n * rows
    whole = [(k * rows, rows) for k in range(n - 2)]
    return whole + [(r, LAST) for r in range((n - 2) * rows, seq, LAST)]


def layer_kernel(
    n, nt, group,
    tok_ref, gain_ref, aq_ref, ak_ref, av_ref, rq_ref, rf_ref, ri_ref, shift_ref,
    wa_ref, wr_ref, offset_ref, bound_ref, rec_gain_ref,
    out_ref,
    tokens, gains, bounds, rec_gains, weights, outs, wide_shift, own_shift, tbuf, shifts, squares, scales,
    part, sent, came, x, state, heads, shares, landed, mixed,
    l_sem, a_send, a_recv, b_send, b_recv, d_send, d_recv, q_send, q_recv,
    c_send, c_recv, e_send, e_recv, f_send, f_recv, g_send, g_recv,
):
    s, t = lax.axis_index("sp"), lax.axis_index("tp")
    rows, feats = own_shift.shape[0], tokens.shape[-1]
    piece = rows // nt
    width = x.shape[1]
    att_width = (group + 2) * HEAD
    wide = group * HEAD
    cols = outs.shape[-1]
    subs = rows // SUB
    ends = (0, n - 1)
    f32, bf16 = jnp.float32, jnp.bfloat16
    units = units_of(n, rows)
    nu = len(units)

    load_tokens = pltpu.make_async_copy(tok_ref, tokens, l_sem.at[0])
    load_gain = pltpu.make_async_copy(
        gain_ref.at[:, pl.ds(pl.multiple_of(s * feats, feats), feats)], gains, l_sem.at[1]
    )
    load_weights = []
    first = 0
    for ref, size in (
        (aq_ref, wide), (ak_ref, HEAD), (av_ref, HEAD),
        (rq_ref, REC_KEY), (rf_ref, REC_KEY), (ri_ref, REC_VAL),
    ):
        for i in range(2):
            load_weights.append(
                pltpu.make_async_copy(
                    ref.at[pl.ds(i * size, size)], weights.at[i, pl.ds(first, size)], l_sem.at[2]
                )
            )
        first += size
    load_shift = pltpu.make_async_copy(shift_ref, wide_shift, l_sem.at[3])
    load_bounds = pltpu.make_async_copy(bound_ref, bounds, l_sem.at[4])
    load_rec_gains = pltpu.make_async_copy(rec_gain_ref, rec_gains, l_sem.at[5])
    load_outs = [
        pltpu.make_async_copy(ref, outs.at[o], l_sem.at[6]) for o, ref in enumerate((wa_ref, wr_ref))
    ]

    load_tokens.start()
    barrier = pltpu.get_barrier_semaphore()
    for a in range(n):
        for b in range(nt):
            if a or b:
                pl.semaphore_signal(
                    barrier, inc=1,
                    device_id={"sp": lax.rem(s + a, n), "tp": lax.rem(t + b, nt)},
                    device_id_type=MESH,
                )
    for load in (
        load_shift, load_gain, *load_weights, load_bounds, load_rec_gains, *load_outs
    ):
        load.start()
    load_tokens.wait()
    with scope("barrier"):
        pl.semaphore_wait(barrier, n * nt - 1)

    def plane(v):
        others = [i for i in range(2) if v != ends[i]]
        mine = [i for i in range(2) if v == ends[i]]
        order = (1, 0) if v < n // 2 else (0, 1)

        def parts_of(k):
            return range(subs) if k == 0 else (slice(None),)

        def slot(c):
            return 0 if isinstance(c, slice) else c

        def lane_of(k, c):
            return c if k == 0 else subs + k - 1

        def first_copy(c, j):
            return remote(
                tokens.at[c, j], tbuf.at[v, c, j], a_send, a_recv.at[lane_of(v, c)],
                {"sp": t, "tp": j},
            )

        def first_here(c):
            return pltpu.make_async_copy(
                tokens.at[c, v], tbuf.at[v, c, v], a_recv.at[lane_of(v, c)]
            )

        def send_first(when):
            pl.when(when)(send_first_now)

        def send_first_now():
            for c in parts_of(v):
                for j in range(nt):
                    if j == v:
                        pl.when(t != v)(lambda: first_copy(c, j).start())
                        pl.when(t == v)(lambda: first_here(c).start())
                    else:
                        first_copy(c, j).start()

        def second_copy(k, c, d):
            return remote(
                tbuf.at[k, c, t], tbuf.at[k, c, t],
                b_send, b_recv.at[lane_of(k, c)],
                {"tp": lax.rem(t + d, nt)},
            )

        def relay(k, c):
            with scope(f"relay{k}"):
                remote(
                    tokens.at[c, 0], tbuf.at[k, c, t], a_send, a_recv.at[lane_of(k, c)],
                    {"sp": (v + 1) % n},
                ).wait_recv()
            for d in range(1, nt):
                second_copy(k, c, d).start()

        def square_copy(k, i):
            return remote(
                squares.at[v, k], squares.at[v, k], q_send.at[i], q_recv.at[k],
                {"sp": ends[i]},
            )

        def chain_copy(i, c):
            to = v - 1 if i == 0 else v + 1
            return remote(
                sent.at[i, pl.ds(c * SUB, SUB)], came.at[i, pl.ds(c * SUB, SUB)],
                c_send.at[i], c_recv.at[i, c], {"sp": to},
            )

        def project(k, c):
            with scope(f"wtok{k}"):
                most = tbuf.at[k, c, pl.ds(0, nt - 1)]
                remote(
                    most, most, b_send, b_recv.at[lane_of(k, c)], {"tp": lax.rem(t + 1, nt)}
                ).wait_recv()
            size = rows if isinstance(c, slice) else SUB
            begin = k * rows + slot(c) * SUB
            raw = tbuf[k, c].reshape(size, feats).astype(f32)
            scaled = (raw * gains[...]).astype(bf16)
            for i in order:
                product = dot_nt(scaled, weights[i])
                if v == ends[1 - i]:
                    for r in range(size // SUB):
                        at = begin + r * SUB
                        sent[i, pl.ds(at, SUB)] = product[r * SUB:(r + 1) * SUB].astype(bf16)
                        chain_copy(i, at // SUB).start()
                else:
                    part[i, pl.ds(begin, size)] = product

        def square(k):
            raw = tbuf[k].reshape(rows, feats).astype(f32)
            total = jnp.sum(raw * raw, axis=1, keepdims=True)
            flat = jnp.transpose(jnp.broadcast_to(total, (rows, 128)))
            squares[v, k] = flat[:8]
            for i in others:
                square_copy(k, i).start()

        def shift_copy(i):
            return remote(
                own_shift.at[:, pl.ds(i * REC_KEY, REC_KEY)], shifts.at[pl.ds(v * rows, rows)],
                d_send.at[i], d_recv.at[v], {"sp": ends[i]},
            )

        def shift_here(i):
            return pltpu.make_async_copy(
                own_shift.at[:, pl.ds(i * REC_KEY, REC_KEY)], shifts.at[pl.ds(v * rows, rows)],
                d_recv.at[v],
            )

        def send_shift(i):
            if v == ends[i]:
                shift_here(i).start()
            else:
                shift_copy(i).start()

        def forward(i, c):
            with scope(f"chain{i}_{c}"):
                chain_copy(i, c).wait_recv()
            at = (i, pl.ds(c * SUB, SUB))
            sent[at] = (part[at] + came[at].astype(f32)).astype(bf16)
            chain_copy(i, c).start()

        def head_copy(i, u, to):
            at = (i, pl.ds(units[u][0], units[u][1]))
            return remote(
                heads.at[at], heads.at[at], e_send.at[to], e_recv.at[i, u], {"sp": to}
            )

        def near(i):
            return 1 if i == 0 else n - 2

        def between(i):
            return [p for p in range(1, n - 1) if p != near(i)]

        def direct(i, u):
            return MODES[i][units[u][0] // rows] == 2

        def relayed(i, u):
            return MODES[i][units[u][0] // rows] == 0

        def head_targets(i, u):
            far = ends[1 - i]
            if relayed(i, u):
                return [] if v == far else [v + 1 if i == 0 else v - 1]
            if v == ends[i]:
                if direct(i, u):
                    return [far, *between(i), near(i)]
                return [near(i), far]
            if v == near(i) and not direct(i, u):
                return between(i)
            return []

        def send_heads(i, u, to):
            head_copy(i, u, to).start()

        def wait_heads(i, u):
            with scope(f"whead{i}_{u}"):
                head_copy(i, u, ends[i]).wait_recv()

        def mix(u):
            e = mine[0]
            begin, size = units[u]
            k = begin // rows
            span = pl.ds(begin, size)
            with scope(f"wmix{u}"):
                for c in range(begin // SUB, (begin + size) // SUB):
                    chain_copy(e, c).wait_recv()
            if begin % rows == 0:
                most = squares.at[pl.ds(0, n - 1), k]
                remote(most, most, q_send.at[e], q_recv.at[k], {"sp": ends[1 - e]}).wait_recv()
                remote(
                    own_shift.at[:, pl.ds(e * REC_KEY, REC_KEY)],
                    shifts.at[pl.ds(k * rows, rows)], d_send.at[e], d_recv.at[k],
                    {"sp": ends[1 - e]},
                ).wait_recv()
                total = squares[0, k, :1]
                for p in range(1, n):
                    total = total + squares[p, k, :1]
                inv_rms = lax.rsqrt(total / (feats * n) + EPS)
                scales[...] = jnp.transpose(jnp.broadcast_to(inv_rms, (128, rows)))
            inv_rms = scales[pl.ds(begin % rows, size)]
            for c in range(width // 128):
                lane = pl.ds(c * 128, 128)
                result = part[e, span, lane] + came[e, span, lane].astype(f32)
                x[span, lane] = (result * inv_rms).astype(bf16)
            with scope(f"stick{u}"):
                heads[e, span, pl.ds(0, wide)] = stick_block(
                    begin, size, e, group, x, offset_ref
                )
            with scope(f"state{u}"):
                heads[e, span, pl.ds(wide, REC_VAL)] = state_block(
                    begin, size, x, att_width,
                    bounds[:, pl.ds(e * REC_KEY, REC_KEY)],
                    rec_gains[:, pl.ds(e * REC_VAL, REC_VAL)], shifts, state,
                )

        def share_copy(k, b):
            to = lax.rem(t + b, nt)
            return remote(
                shares.at[k, to], landed.at[k, b], f_send, f_recv.at[k], {"tp": to}
            )

        def multiply(u):
            begin, size = units[u]
            k = begin // rows
            span = pl.ds(begin, size)
            total = None
            for i in range(2):
                for o, at, deep in ((0, 0, wide), (1, wide, REC_VAL)):
                    term = dot_nn(heads[i, span, pl.ds(at, deep)], outs[o, pl.ds(i * deep, deep)])
                    total = term if total is None else total + term
            total = total.astype(bf16)
            if size == rows:
                shares[k] = total.reshape(nt, piece, cols)
                for b in range(1, nt):
                    share_copy(k, b).start()
            else:
                for j in range(begin % rows // piece, (begin % rows + size) // piece):
                    at = j * piece - begin % rows
                    shares[k, j] = total[at:at + piece]
                    b = lax.rem(j - t + nt, nt)
                    pl.when(t != j)(lambda: share_copy(k, b).start())

        place = out_ref.at[:, pl.ds(v * cols, cols)]

        def final_copy(k):
            return remote(mixed.at[k], place, g_send, g_recv, {"sp": k})

        def final_here():
            return pltpu.make_async_copy(mixed.at[v], place, g_recv)

        def combine(k):
            with scope(f"wshare{k}"):
                most = pl.ds(1, nt - 1)
                remote(
                    shares.at[k, most], landed.at[k, most], f_send, f_recv.at[k],
                    {"tp": lax.rem(t + 1, nt)},
                ).wait_recv()
            result = shares[k, t].astype(f32)
            for b in range(1, nt):
                result = result + landed[k, b].astype(f32)
            mixed[k] = result.astype(bf16)
            if k == v:
                final_here().start()
            else:
                final_copy(k).start()

        def projection_loaded():
            load_gain.wait()
            pltpu.make_async_copy(weights, weights, l_sem.at[2]).wait()

        def rest_loaded():
            load_bounds.wait()
            load_rec_gains.wait()
            pltpu.make_async_copy(outs, outs, l_sem.at[6]).wait()

        events = []

        def event(time, *call):
            events.append((time, len(events), call))

        starts = (START0, START1)
        hops = (n - 1 - v, v)
        whole = slice(None)
        event(5.9, projection_loaded)
        def round_shift():
            own_shift[...] = wide_shift[...].astype(bf16)

        event(0.1, load_shift.wait)
        event(0.15, round_shift)
        event(15.0, rest_loaded)
        soon = t < v
        if v < n // 2:
            soon = soon | (t == n - 1)
        if v == 0:
            soon = t >= 0
        event(0.0, send_first, soon)
        for c in range(subs):
            event(4.0 + 0.1 * c, relay, 0, c)
        event(4.05, send_first, jnp.logical_not(soon))
        for c in range(subs):
            event(6.0 + 0.1 * c, project, 0, c)
        event(0.2, send_shift, 0)
        event(4.4 if 0 < v < n - 1 else 0.2, send_shift, 1)
        event(7.1, square, 0)
        ready = [6.5]
        for k in range(1, n):
            event(6.05 if k == 1 else 9.0 + 0.1 * k, relay, k, whole)
            at = (TOKENS if v in ends else TOKENS_MID)[k - 1]
            event(at, project, k, whole)
            event(at + 0.1, square, k)
            ready.append(at + 0.01)
        chain_end = 0.0
        if v not in ends:
            for i in range(2):
                for c in range(n * subs):
                    at = max(starts[i] + hops[i] * HOP + CHUNK * c, ready[c // subs])
                    event(at, forward, i, c)
                    chain_end = max(chain_end, at)
        def distance(i, p):
            return p if i == 0 else n - 1 - p

        def leaves(i, u, to):
            last = starts[1 - i] + distance(i, to) * HOP + CHUNK * (n * subs - 1)
            return max(done[i][u] - 0.1, last - FAR)

        done = [[0.0] * nu, [0.0] * nu]
        for i in range(2):
            at = 0.0
            for u, (begin, size) in enumerate(units):
                last = (begin + size) // SUB - 1
                arrive = max(at, starts[i] + (n - 1) * HOP + CHUNK * last)
                at = arrive + (1.8 if size == rows else 1.45)
                done[i][u] = at
                if v == ends[i]:
                    event(arrive, mix, u)
                    for to in head_targets(i, u):
                        event(leaves(i, u, to), send_heads, i, u, to)
        for u, (begin, size) in enumerate(units):
            k = begin // rows
            latest = max(done[0][u], done[1][u], chain_end + 0.01)
            for i in others:
                load = 1.4 * size / rows
                away = distance(i, v)
                if relayed(i, u):
                    at = leaves(i, u, near(i)) + (3.0 + load) * away
                elif direct(i, u):
                    at = leaves(i, u, v) + 2.8 + 0.45 * away + (n - away) * load
                elif v in between(i):
                    at = leaves(i, u, near(i)) + 6.5 + 2 * load
                else:
                    at = leaves(i, u, v) + 2.8 + 0.45 * away + load
                if v in ends:
                    at = max(at, done[mine[0]][nu - 1] + 0.01)
                elif v == 1 and i == 0 and relayed(i, u):
                    at -= 0.2
                else:
                    at = max(at, chain_end + 0.01)
                event(at, wait_heads, i, u)
                for to in head_targets(i, u):
                    event(at, send_heads, i, u, to)
                latest = max(latest, at)
            event(latest + 0.02, multiply, u)
            if begin + size == (k + 1) * rows:
                event(latest + 6.0, combine, k)
        for _, _, (call, *args) in sorted(events, key=lambda e: e[:2]):
            call(*args)

        with scope("wfinal"):
            pltpu.make_async_copy(out_ref, out_ref, g_recv).wait()

        with scope("wsend"):
            def sent_all(src, sem):
                remote(src, src, sem, a_recv.at[0], {"sp": (v + 1) % n}).wait_send()

            pl.when(t != v)(lambda: sent_all(tokens, a_send))
            pl.when(t == v)(lambda: sent_all(tokens.at[:, pl.ds(0, nt - 1)], a_send))
            sent_all(tbuf.at[:, :, pl.ds(0, nt - 1)], b_send)
            sent_all(shares.at[:, pl.ds(0, nt - 1)], f_send)
            sent_all(mixed.at[pl.ds(0, n - 1)], g_send)
            for i in others:
                sent_all(own_shift.at[:, pl.ds(i * REC_KEY, REC_KEY)], d_send.at[i])
                sent_all(squares.at[v], q_send.at[i])
                sent_all(sent.at[i], c_send.at[i])
            for to in range(n):
                spans = [
                    units[u] for i in range(2) for u in range(nu) if to in head_targets(i, u)
                ]
                if spans:
                    begin = spans[0][0]
                    size = sum(size for _, size in spans)
                    sent_all(heads.at[0, pl.ds(begin, size)], e_send.at[to])

    for v in range(n):
        if v in ends:
            @pl.when(s == v)
            def _():
                x[...] = jnp.zeros_like(x)
                plane(v)
        else:
            pl.when(s == v)(functools.partial(plane, v))


START0, START1, HOP, CHUNK = 8.4, 6.3, 3.6, 0.88
FAR = 3.2
MODES = ((0, 1, 1, 1), (0, 0, 1, 1))
TOKENS = (10.5, 11.5, 12.5)
TOKENS_MID = (10.5, 14.0, 16.5)


def stationary_fits(args):
    n, nt = lax.axis_size("sp"), lax.axis_size("tp")
    tokens, att_q, att_k, rec_i = args[0], args[2], args[3], args[7]
    rows, feats = tokens.shape
    return (
        n == nt
        and n >= 3
        and att_k.shape[0] // HEAD == 2
        and rec_i.shape[0] // REC_VAL == 2
        and (att_q.shape[0] // att_k.shape[0]) * HEAD == 128
        and feats == att_q.shape[1]
        and rows == 128
        and rows == SUB * nt
        and SUB == ROWS8 * nt
    )


def stationary(*args):
    n, nt = lax.axis_size("sp"), lax.axis_size("tp")
    tokens, norm_gain, att_q, att_k = args[:4]
    score_offset, lower_bound, decay_shift, rec_gain = args[10:]
    rows, feats = tokens.shape
    seq = rows * n
    deep, cols = args[8].shape
    group = att_q.shape[0] // att_k.shape[0]
    width = (group + 2) * HEAD + 2 * REC_KEY + REC_VAL
    wide = group * HEAD + REC_VAL
    piece = rows // nt
    chunks = seq // SUB
    subs = rows // SUB
    nu = len(units_of(n, rows))
    bf16, f32 = jnp.bfloat16, jnp.float32
    dma = pltpu.SemaphoreType.DMA
    vmem = pl.BlockSpec(memory_space=pltpu.VMEM)
    hbm = pl.BlockSpec(memory_space=pl.ANY)
    smem = pl.BlockSpec(memory_space=pltpu.SMEM)
    return pl.pallas_call(
        functools.partial(layer_kernel, n, nt, group),
        out_shape=pltpu.VMEM((piece, cols * n), bf16),
        in_specs=[hbm] * 11 + [smem, hbm, hbm],
        out_specs=vmem,
        scratch_shapes=[
            pltpu.VMEM((subs, nt, ROWS8, feats), bf16),
            pltpu.VMEM((1, feats), f32),
            pltpu.VMEM((1, 2 * REC_KEY), f32),
            pltpu.VMEM((1, 2 * REC_VAL), f32),
            pltpu.VMEM((2, width, feats), bf16),
            pltpu.VMEM((2, deep, cols), bf16),
            pltpu.VMEM((rows, 2 * REC_KEY), f32),
            pltpu.VMEM((rows, 2 * REC_KEY), bf16),
            pltpu.VMEM((n, subs, nt, ROWS8, feats), bf16),
            pltpu.VMEM((seq, REC_KEY), bf16),
            pltpu.VMEM((n, n, 8, rows), f32),
            pltpu.VMEM((rows, 128), f32),
            pltpu.VMEM((2, seq, width), f32),
            pltpu.VMEM((2, seq, width), bf16),
            pltpu.VMEM((2, seq, width), bf16),
            pltpu.VMEM((seq, width), bf16),
            pltpu.VMEM((REC_VAL, REC_KEY), f32),
            pltpu.VMEM((2, seq, wide), bf16),
            pltpu.VMEM((n, nt, piece, cols), bf16),
            pltpu.VMEM((n, nt, piece, cols), bf16),
            pltpu.VMEM((n, piece, cols), bf16),
            dma((7,)), dma, dma((subs + n - 1,)), dma, dma((subs + n - 1,)), dma((2,)), dma((n,)),
            dma((2,)), dma((n,)), dma((2,)), dma((2, chunks)), dma((n,)), dma((2, nu)),
            dma, dma((n,)), dma, dma,
        ],
        compiler_params=pltpu.CompilerParams(collective_id=0, has_side_effects=True),
        name="layer",
    )(
        tokens.reshape(subs, nt, ROWS8, feats), norm_gain.reshape(1, -1), *args[2:8], decay_shift,
        args[8], args[9],
        score_offset, lower_bound.reshape(1, -1), rec_gain.reshape(1, -1),
    )


def on_device(*args):
    if stationary_fits(args):
        return stationary(*args)
    return gathered_plan(*args)


def solution(mesh):
    in_specs = (
        P(("grp", "sp"), "tp"),
        P(),
        P("tp", "sp"),
        P("tp", "sp"),
        P("tp", "sp"),
        P("tp", "sp"),
        P("tp", "sp"),
        P("tp", "sp"),
        P("tp", "sp"),
        P("tp", "sp"),
        P("tp"),
        P("tp"),
        P(("grp", "sp"), "tp"),
        P("tp"),
    )
    out_specs = P(("grp", "sp", "tp"), None)
    return jax.shard_map(
        on_device, mesh=mesh, in_specs=in_specs, out_specs=out_specs, check_vma=False
    )
```
